32 devices in a mesh: sp: 8 (over z, y), tp: 4 (over x, core).
Axes of the slice: x: 2, y: 2, z: 4, core: 2. Of those that a mesh axis runs over, the one named last changes fastest.
Arguments:
- hidden: bfloat16 [2048, 4096], P('sp'), as said below
- key_weight: bfloat16 [4096, 1024], P(None, 'tp'), as said below
- queries: bfloat16 [2048, 4096], P('sp', 'tp'), as said below
- values: bfloat16 [2048, 1024], P('sp', 'tp'), as said below
- map_out: bfloat16 [2048, 8192], P('sp', 'tp'), as said below
- log_sums: float32 [32, 2048], P('tp', 'sp'), as said below
- out_grad: bfloat16 [2048, 4096], P('sp', 'tp'), may hold values from -6 to 6
- mixing: float32 [16], P('tp'), may hold values from 0.3 to 0.8
- out_gain: float32 [256], replicated, may hold values from 0.1 to 1.9
Outputs:
- grad_query: bfloat16 [2048, 4096], P('sp', 'tp')
- grad_key: bfloat16 [2048, 1024], P('sp', 'tp')
- grad_value: bfloat16 [2048, 1024], P('sp', 'tp')
- grad_weight: float32 [4096, 1024], P('sp', 'tp')
The draws below stay inside these ranges and needn't reach their ends.
Inputs may be any that keep to these rules, and one draw needn't show every extreme that they name: `hidden`: inputs of order one. `key_weight`: entries of order 1 / sqrt(4096) times a constant. `queries`: entries of order one. `values`: entries of order one. `log_sums`: for head h, map m and row i: the logarithm of the sum over keys j <= i of exp(scores[h, m](i, j)), with key_rows formed as in the reference program. `map_out`: for head h and map m: the row's weights exp(scores - log_sums) over keys j <= i times the values of key head g(h), rounded to bfloat16.
All inputs are finite; a program needn't handle non-finite values.
Results may differ from the reference program's by a relative error of at most 0.02.
Values may be sent and summed in bfloat16 or wider, within the bound.
A program may use at most 256 MiB of HBM per device.

```python
import math
import jax
import jax.numpy as jnp
from jax import lax

D = 4096
HEADS = 16
KV_HEADS = 4
HEAD_DIM = 128
V_DIM = 256
TOKENS = 2048


def base_arrays(key):
    key_hidden = jax.random.fold_in(key, 101)
    key_weight = jax.random.fold_in(key, 102)
    key_query = jax.random.fold_in(key, 103)
    key_value = jax.random.fold_in(key, 104)
    hidden = jax.random.normal(key_hidden, (TOKENS, D), jnp.float32)
    queries = jax.random.normal(key_query, (TOKENS, HEADS * 2 * HEAD_DIM), jnp.float32)
    weight = jax.random.normal(key_weight, (D, KV_HEADS * 2 * HEAD_DIM), jnp.float32) * (1.5 / math.sqrt(D))
    values = jax.random.normal(key_value, (TOKENS, KV_HEADS * V_DIM), jnp.float32)
    return (hidden.astype(jnp.bfloat16), weight.astype(jnp.bfloat16), queries.astype(jnp.bfloat16), values.astype(jnp.bfloat16))


def forward_arrays(key):
    hidden, weight, queries, values = base_arrays(key)
    key_rows = jnp.dot(hidden, weight, preferred_element_type=jnp.float32).astype(jnp.bfloat16).astype(jnp.float32)
    per_group = HEADS // KV_HEADS
    block_rows = 128 if TOKENS % 128 == 0 else TOKENS
    n_blocks = TOKENS // block_rows
    query_all = queries.astype(jnp.float32).reshape(n_blocks, block_rows, KV_HEADS, per_group, 2, HEAD_DIM)
    key_all = key_rows.reshape(TOKENS, KV_HEADS, 2, HEAD_DIM)
    value_all = values.astype(jnp.float32).reshape(TOKENS, KV_HEADS, V_DIM)
    positions = jnp.arange(TOKENS, dtype=jnp.int32).reshape(n_blocks, block_rows)
    key_pos = jnp.arange(TOKENS, dtype=jnp.int32)
    sums_list, outs_list = ([], [])
    for head_group in range(KV_HEADS):
        key_g = key_all[:, head_group]
        value_g = value_all[:, head_group]

        def one_block(inputs):
            query_block, query_pos = inputs
            scores = jnp.einsum('bpmd,tmd->pmbt', query_block[:, head_group], key_g) * HEAD_DIM ** (-0.5)
            visible = key_pos[None, :] <= query_pos[:, None]
            scores = jnp.where(visible, scores, -1e+30)
            row_max = jnp.max(scores, axis=-1, keepdims=True)
            log_sum = row_max + jnp.log(jnp.sum(jnp.exp(scores - row_max), axis=-1, keepdims=True))
            probs_map = jnp.exp(scores - log_sum)
            outputs = jnp.einsum('pmbt,tv->bpmv', probs_map, value_g)
            return (log_sum[..., 0], outputs)
        sums_g, outs_g = lax.map(one_block, (query_all, positions))
        sums_list.append(jnp.transpose(sums_g, (1, 2, 0, 3)).reshape(per_group * 2, TOKENS))
        outs_list.append(outs_g.reshape(TOKENS, per_group * 2 * V_DIM))
    return (jnp.concatenate(sums_list, axis=0), jnp.concatenate(outs_list, axis=1).astype(jnp.bfloat16))


def draw_hidden(key, part):
    return base_arrays(key)[0]


def draw_key_weight(key, part):
    return base_arrays(key)[1]


def draw_queries(key, part):
    return base_arrays(key)[2]


def draw_values(key, part):
    return base_arrays(key)[3]


def draw_log_sums(key, part):
    return forward_arrays(key)[0]


def draw_map_out(key, part):
    return forward_arrays(key)[1]


def spiked(entries, stream_key, source, target, blocks, factor):
    def block_of(axis_at):
        return (jnp.arange(entries.shape[axis_at]) // (entries.shape[axis_at] // blocks)).reshape((-1,) + (1,) * (entries.ndim - 1 - axis_at))

    first = jax.random.permutation(stream_key, blocks)[block_of(target)]
    second = (block_of(target) + blocks // 2) % blocks
    return jnp.where((block_of(source) == first) | (block_of(source) == second), factor * entries, entries)


def steps_of(stream_key, shape, cuts, smallest, high):
    def one(dim, blocks):
        heights = jax.random.uniform(jax.random.fold_in(jax.random.fold_in(stream_key, 6), dim), (blocks,), jnp.float32, smallest / len(cuts), high / len(cuts))
        return jnp.repeat(jnp.exp(heights), shape[dim] // blocks).reshape((-1,) + (1,) * (len(shape) - dim - 1))

    level = one(*cuts[0])
    for cut in cuts[1:]:
        level = level * one(*cut)
    return level


def bell_draw_with(own_key, extent, deviation, most, cuts, heavy, held_as=jnp.bfloat16):
    entries = deviation * jax.random.normal(own_key, extent, jnp.float32)
    if cuts:
        entries = entries * steps_of(own_key, extent, cuts, -0.22, 0.18)
    return jnp.clip(spiked(entries, jax.random.fold_in(own_key, 3), *heavy), -most, most).astype(held_as)


def setup_inputs(seed: int = 0) -> dict:
    seeds = jax.random.split(jax.random.key(seed), 10)
    hidden = draw_hidden(jax.random.fold_in(seeds[9], 71), 0)
    key_weight = draw_key_weight(jax.random.fold_in(seeds[9], 71), 0)
    queries = draw_queries(jax.random.fold_in(seeds[9], 71), 0)
    values = draw_values(jax.random.fold_in(seeds[9], 71), 0)
    map_out = draw_map_out(jax.random.fold_in(seeds[9], 71), 0)
    log_sums = draw_log_sums(jax.random.fold_in(seeds[9], 71), 0)
    out_grad = bell_draw_with(seeds[6], (TOKENS, HEADS * V_DIM), 1.0, 6.0, ((0, 8), (1, 4)), (0, 1, 8, 2.0))
    mixing = jnp.clip(0.3 + 0.5 * jax.random.uniform(seeds[7], (HEADS,), jnp.float32) ** steps_of(seeds[7], (HEADS,), ((0, 4),), -0.2, 0.2), 0.3, 0.8)
    out_gain = jnp.clip(1.0 + 0.18 * jax.random.normal(seeds[8], (V_DIM,), jnp.float32), 0.1, 1.9)
    return {"hidden": hidden, "key_weight": key_weight, "queries": queries, "values": values, "map_out": map_out, "log_sums": log_sums, "out_grad": out_grad, "mixing": mixing, "out_gain": out_gain}


OUT_SCALE = 0.8
NORM_EPS = 1e-06

def head_terms(out_grad, map_out, mixing, out_gain):
    rows_here = out_grad.shape[0]
    heads_here = mixing.shape[0]
    v_width = out_gain.shape[0]
    maps_out = map_out.astype(jnp.float32).reshape(rows_here, heads_here, 2, v_width)
    pre_norm = maps_out[:, :, 0] - mixing[None, :, None] * maps_out[:, :, 1]
    inverse = lax.rsqrt(lax.optimization_barrier(jnp.mean(pre_norm * pre_norm, axis=-1, keepdims=True)) + NORM_EPS)
    upstream = out_grad.astype(jnp.float32).reshape(rows_here, heads_here, v_width) * out_gain * OUT_SCALE
    d_out = inverse * (upstream - pre_norm * inverse * inverse * lax.optimization_barrier(jnp.mean(upstream * pre_norm, axis=-1, keepdims=True)))
    row_terms = lax.optimization_barrier(jnp.sum(d_out[:, :, None, :] * maps_out, axis=-1)).reshape(rows_here, heads_here * 2)
    return (d_out.reshape(rows_here, heads_here * v_width).astype(jnp.bfloat16), row_terms)

def round_trip(array):
    return lax.optimization_barrier(array.astype(jnp.bfloat16)).astype(jnp.float32)

def block_grads(query_blk, d_blk, log_blk, term_blk, query_pos, key_all, value_all, key_pos, mix_blk):
    scale = query_blk.shape[-1] ** (-0.5)
    log_part = jnp.transpose(log_blk, (1, 2, 3, 0))[..., None]
    term_part = jnp.transpose(term_blk, (1, 2, 3, 0))[..., None]
    scores = jnp.einsum('rgpmd,kgmd->gpmrk', query_blk, key_all) * scale
    visible = key_pos[None, :] <= query_pos[:, None]
    probs_map = jnp.exp(jnp.where(visible, scores - log_part, -1e+30))
    d_attn = jnp.einsum('rgpv,kgv->gprk', d_blk, value_all)
    mix_cols = mix_blk[:, :, None, None]
    weights_a = round_trip(probs_map[:, :, 0] - mix_cols * probs_map[:, :, 1])
    d_scores = round_trip(jnp.stack([probs_map[:, :, 0] * (d_attn - term_part[:, :, 0]), -mix_cols * probs_map[:, :, 1] * (d_attn - term_part[:, :, 1])], axis=2))
    grad_q = jnp.einsum('gpmrk,kgmd->rgpmd', d_scores, key_all) * scale
    grad_k = jnp.einsum('gpmrk,rgpmd->kgmd', d_scores, query_blk) * scale
    grad_v = jnp.einsum('gprk,rgpv->kgv', weights_a, d_blk)
    return (grad_q, grad_k, grad_v)

def reference(hidden, key_weight, queries, values, map_out, log_sums, out_grad, mixing, out_gain):
    total = queries.shape[0]
    per_group = HEADS // KV_HEADS
    key_rows = jnp.dot(hidden, key_weight, preferred_element_type=jnp.float32).astype(jnp.bfloat16)
    d_rows, row_terms = head_terms(out_grad, map_out, mixing, out_gain)
    query_all = queries.astype(jnp.float32).reshape(total, KV_HEADS, per_group, 2, HEAD_DIM)
    key_all = key_rows.astype(jnp.float32).reshape(total, KV_HEADS, 2, HEAD_DIM)
    value_all = values.astype(jnp.float32).reshape(total, KV_HEADS, V_DIM)
    d_all = d_rows.astype(jnp.float32).reshape(total, KV_HEADS, per_group, V_DIM)
    log_all = log_sums.T.reshape(total, KV_HEADS, per_group, 2)
    term_all = row_terms.reshape(total, KV_HEADS, per_group, 2)
    mix_all = mixing.reshape(KV_HEADS, per_group)
    block_rows = 256 if total % 256 == 0 else total
    n_blocks = total // block_rows
    key_pos = jnp.arange(total, dtype=jnp.int32)
    query_list, key_list, value_list = ([], [], [])
    for head_group in range(KV_HEADS):
        query_g = query_all[:, head_group:head_group + 1]
        d_g = d_all[:, head_group:head_group + 1]
        log_g = log_all[:, head_group:head_group + 1]
        term_g = term_all[:, head_group:head_group + 1]
        key_g = key_all[:, head_group:head_group + 1]
        value_g = value_all[:, head_group:head_group + 1]
        mix_g = mix_all[head_group:head_group + 1]

        def step_fn(carry, index):
            acc_key, acc_value = carry
            start = (index * block_rows).astype(jnp.int32)
            query_pos = start + jnp.arange(block_rows, dtype=jnp.int32)
            grad_q, grad_k, grad_v = block_grads(lax.dynamic_slice_in_dim(query_g, start, block_rows, 0), lax.dynamic_slice_in_dim(d_g, start, block_rows, 0), lax.dynamic_slice_in_dim(log_g, start, block_rows, 0), lax.dynamic_slice_in_dim(term_g, start, block_rows, 0), query_pos, key_g, value_g, key_pos, mix_g)
            return ((acc_key + grad_k, acc_value + grad_v), grad_q)
        init = (jnp.zeros((total, 1, 2, HEAD_DIM), jnp.float32), jnp.zeros((total, 1, V_DIM), jnp.float32))
        (acc_key, acc_value), grads_q = lax.scan(step_fn, init, jnp.arange(n_blocks, dtype=jnp.int32))
        query_list.append(grads_q.reshape(total, per_group * 2 * HEAD_DIM))
        key_list.append(acc_key.reshape(total, 2 * HEAD_DIM))
        value_list.append(acc_value.reshape(total, V_DIM))
    grad_query = jnp.concatenate(query_list, axis=1).astype(jnp.bfloat16)
    grad_key = jnp.concatenate(key_list, axis=1).astype(jnp.bfloat16)
    grad_value = jnp.concatenate(value_list, axis=1).astype(jnp.bfloat16)
    grad_weight = lax.dot_general(hidden, grad_key, (((0,), (0,)), ((), ())), preferred_element_type=jnp.float32)
    return (grad_query, grad_key, grad_value, grad_weight)
```

```python
import functools
import math

import jax
import jax.numpy as jnp
from jax import lax
from jax.experimental import pallas as pl
from jax.experimental.pallas import tpu as pltpu
from jax.sharding import PartitionSpec as P

HEAD_DIM = 128
V_DIM = 256
OUT_SCALE = 0.8
NORM_EPS = 1e-06
LOG2E = math.log2(math.e)
SCALE = HEAD_DIM ** (-0.5)
VMEM = pltpu.VMEM
DMA = pltpu.SemaphoreType.DMA


def dot_nn(a, b):
    return lax.dot_general(a, b, (((1,), (0,)), ((), ())), preferred_element_type=jnp.float32)


def dot_nt(a, b):
    return lax.dot_general(a, b, (((1,), (1,)), ((), ())), preferred_element_type=jnp.float32)


def dot_tn(a, b):
    return lax.dot_general(a, b, (((0,), (0,)), ((), ())), preferred_element_type=jnp.float32)


def head_terms(pair, half, slot, og_ref, mo_ref, log_ref, mix_ref, gain_ref, d_ref, m_ref):
    gain = gain_ref[...] * OUT_SCALE
    rows = og_ref.shape[0]
    cols, lifts = [], []
    for i in range(half):
        h = pair * half + i
        at = pl.multiple_of(2 * h * V_DIM, V_DIM)
        map_a = mo_ref[:, pl.ds(at, V_DIM)].astype(jnp.float32)
        map_b = mo_ref[:, pl.ds(at + V_DIM, V_DIM)].astype(jnp.float32)
        pre = map_a - mix_ref[h] * map_b
        inv = lax.rsqrt(jnp.mean(pre * pre, axis=-1, keepdims=True) + NORM_EPS)
        up = og_ref[:, pl.ds(pl.multiple_of(h * V_DIM, V_DIM), V_DIM)].astype(jnp.float32) * gain
        d_out = inv * (up - pre * (inv * inv * jnp.mean(up * pre, axis=-1, keepdims=True)))
        d_ref[slot, :, i * V_DIM : (i + 1) * V_DIM] = d_out.astype(jnp.bfloat16)
        cols.append(jnp.sum(d_out * map_a, axis=-1, keepdims=True))
        cols.append(jnp.sum(d_out * map_b, axis=-1, keepdims=True))
        lifts.append(jnp.zeros((1, rows), jnp.float32))
        lifts.append(jnp.log(jnp.full((1, rows), mix_ref[h], jnp.float32)))
    lane = lax.broadcasted_iota(jnp.int32, (rows, 128), 1)
    packed = jnp.zeros((rows, 128), jnp.float32)
    for at, col in enumerate(cols):
        packed = jnp.where(lane == at, col, packed)
    logs = log_ref[...]
    logs = jnp.where(pair == 0, logs[: 2 * half], logs[2 * half :])
    m_ref[slot, : 2 * half] = (logs - jnp.concatenate(lifts, axis=0)) * LOG2E
    m_ref[slot, 2 * half :] = packed.T[: 2 * half]


def block_grads(half, slots, k_ref, v_ref, q_ref, d_ref, m_ref, gq_ref, masked):
    keys = [k_ref[:, m * HEAD_DIM : (m + 1) * HEAD_DIM] for m in range(2)]
    keys_t = [k.T for k in keys]
    vals = v_ref[...]
    grad_k = [None, None]
    grad_v = None
    for slot in slots:
        for i in range(half):
            d_h = d_ref[slot, :, i * V_DIM : (i + 1) * V_DIM]
            d_attn = dot_nt(vals, d_h)
            qs, probs, terms = [], [], []
            for m in range(2):
                at = 2 * i + m
                q = q_ref[slot, :, at * HEAD_DIM : (at + 1) * HEAD_DIM]
                p = jnp.exp2(dot_nt(keys[m], q) * (SCALE * LOG2E) - m_ref[slot, at : at + 1, :])
                if masked:
                    k_at = lax.broadcasted_iota(jnp.int32, p.shape, 0)
                    q_at = lax.broadcasted_iota(jnp.int32, p.shape, 1)
                    p = jnp.where(k_at <= q_at, p, 0.0)
                qs.append(q)
                probs.append(p)
                terms.append(m_ref[slot, 2 * half + at : 2 * half + at + 1, :])
            w = (probs[0] - probs[1]).astype(jnp.bfloat16)
            ds = [
                (probs[0] * (d_attn - terms[0])).astype(jnp.bfloat16),
                (probs[1] * (terms[1] - d_attn)).astype(jnp.bfloat16),
            ]
            for m in range(2):
                at = 2 * i + m
                gq_ref[slot, at * HEAD_DIM : (at + 1) * HEAD_DIM, :] += dot_nn(keys_t[m], ds[m])
                gk = dot_nn(ds[m], qs[m])
                grad_k[m] = gk if grad_k[m] is None else grad_k[m] + gk
            gv = dot_nn(w, d_h)
            grad_v = gv if grad_v is None else grad_v + gv
    return grad_k, grad_v


def attend_kernel(
    n, tp_count, heads,
    hidden_ref, weight_ref, values_ref, q_in_ref, mo_in_ref, og_in_ref, log_ref, gain_ref, mix_ref,
    gq_out, gk_out, gv_out, gw_out,
    hid_vm, w_vm, mo_vm, og_vm, qb, db, mb, kv, acc, keep, p_out, p_in, up_in, dn_out,
    gkb, gv_fin, gv_in, gq_t, gq_fin, gq_in, hid,
    load_sem, q_send, q_recv, d_send, d_recv, m_send, m_recv,
    kv_recv, kv_own, kv_up, kv_pair, p_send, p_recv, dn_send, up_recv,
    gk_recv, gk_up, gk_dn, gk_pair, gk_cross, gv_send, gv_recv, gq_send, gq_recv,
    hid_send, hid_recv, hid_pass, hid_pair,
):
    me = lax.axis_index("sp")
    tp = lax.axis_index("tp")
    outer = n // 2
    half = heads // 2
    o, y = me // 2, me % 2
    x, c = tp // 2, tp % 2
    mate, pair = me + 1 - 2 * y, tp + 1 - 2 * c
    has_up = o < outer - 1
    home = y == c
    rows = og_in_ref.shape[0]
    hrows = rows // 2
    pair_q, pair_v = half * 2 * HEAD_DIM, half * V_DIM

    def remote(src, dst, send, recv, sp=me, to=tp):
        return pltpu.make_async_remote_copy(
            src_ref=src, dst_ref=dst, send_sem=send, recv_sem=recv, device_id={"sp": sp, "tp": to}
        )

    def landed(ref, sem):
        pltpu.make_async_copy(ref, ref, sem).wait()

    own_kv = jnp.where(home, me, n)

    def slot_of(p):
        return jnp.where(home & (p == c), y, 2 + p)

    def load(k):
        if k < 2:
            return pltpu.make_async_copy(
                q_in_ref.at[:, pl.ds(k * pair_q, pair_q)], qb.at[slot_of(k)], load_sem.at[k]
            )
        src, dst = {
            2: (values_ref, kv.at[own_kv, 1]),
            3: (hidden_ref, hid_vm),
            4: (weight_ref, w_vm),
            5: (mo_in_ref, mo_vm),
            6: (og_in_ref, og_vm),
        }[k]
        return pltpu.make_async_copy(src, dst, load_sem.at[k])

    for k in (2, 3, 4, 0, 1, 5, 6):
        load(k).start()

    barrier = pltpu.get_barrier_semaphore()

    @pl.loop(1, n)
    def _(k):
        pl.semaphore_signal(barrier, inc=1, device_id={"sp": (me + k) % n})

    @pl.loop(1, tp_count)
    def _(k):
        pl.semaphore_signal(barrier, inc=1, device_id={"tp": (tp + k) % tp_count})

    pl.semaphore_signal(barrier, inc=1, device_id={"sp": mate, "tp": pair})
    pl.semaphore_wait(barrier, n + tp_count - 1)

    def spread(buf, p, send, recv):
        return remote(buf.at[2 + p], buf.at[y], send.at[p], recv.at[y], 2 * o + c, 2 * x + p)

    def not_self(p):
        return ~(home & (p == c))

    def arrive(buf, slot, recv):
        landed(buf.at[slot], recv.at[slot])

    def rows_arrive(slot):
        arrive(qb, slot, q_recv)
        arrive(db, slot, d_recv)
        arrive(mb, slot, m_recv)

    def own_copy(p):
        return remote(
            kv.at[own_kv, p], kv.at[me, p], kv_own.at[p], kv_recv.at[me, p],
            2 * o + c, 2 * x + jnp.where(home, 1 - c, p),
        )

    def up_copy(b):
        return remote(kv.at[b, c], kv.at[b, c], kv_up.at[b], kv_recv.at[b, c], me + 2)

    def pair_copy(b):
        return remote(kv.at[b, c], kv.at[b, c], kv_pair.at[b], kv_recv.at[b, c], me, pair)

    def kv_wait(b, p):
        landed(kv.at[b, p], kv_recv.at[b, p])

    def pass_up(b):
        @pl.when(has_up)
        def _():
            up_copy(b).start()

    def take(b):
        kv_wait(b, c)
        pass_up(b)
        pair_copy(b).start()

    part_rows = rows // tp_count
    wide = hid_vm.shape[1] // n
    own_rows = pl.ds(pl.multiple_of(tp * part_rows, part_rows), part_rows)

    def columns(dest):
        return pl.ds(pl.multiple_of(dest * wide, wide), wide)

    def hid_slice(dest):
        return remote(hid_vm.at[own_rows, columns(dest)], hid.at[tp, me], hid_send, hid_recv.at[tp], dest)

    def hid_early():
        @pl.loop(0, o)
        def _(l):
            hid_slice(2 * l + y).start()

    def hid_late():
        @pl.loop(1, n)
        def _(k):
            dest = (me + k) % n

            @pl.when((dest // 2 >= o) | (dest % 2 != y))
            def _():
                hid_slice(dest).start()

    def hid_wait(sem):
        pieces = hid.at[tp, pl.ds(0, n - 1)]
        pltpu.make_async_copy(pieces, pieces, sem).wait()

    def hid_over(k):
        return remote(hid.at[tp], hid.at[tp], hid_pass.at[k], hid_recv.at[tp], me, (tp + 2 * k) % tp_count)

    def hid_to_pair(k):
        source = (tp + 2 * k) % tp_count
        return remote(hid.at[source], hid.at[source], hid_pair.at[k], hid_recv.at[source], me, pair)

    load(2).wait()
    own_copy(1).start()

    @pl.when(home & (c == 1) & has_up)
    def _():
        up_copy(me).start()

    for p in range(2):
        load(p).wait()

    def send_q(p):
        @pl.when(not_self(p))
        def _():
            spread(qb, p, q_send, q_recv).start()

    send_q(0)
    load(3).wait()
    load(4).wait()
    kv[own_kv, 0] = dot_nn(hid_vm[...], w_vm[...]).astype(jnp.bfloat16)
    own_copy(0).start()

    @pl.when(home & (c == 0) & has_up)
    def _():
        up_copy(me).start()

    send_q(1)
    load(5).wait()
    load(6).wait()

    @pl.loop(0, 2)
    def _(k):
        p = jnp.where(k == 0, 1 - c, c)
        head_terms(p, half, slot_of(p), og_vm, mo_vm, log_ref, mix_ref, gain_ref, db, mb)

        @pl.when(not_self(p))
        def _():
            spread(db, p, d_send, d_recv).start()
            spread(mb, p, m_send, m_recv).start()

    hid[tp, me] = hid_vm[own_rows, columns(me)]
    hid_early()
    gw_out[...] = jnp.zeros_like(gw_out)
    gq_t[...] = jnp.zeros_like(gq_t)

    def grads(b, slots, masked=False):
        grad_k, grad_v = block_grads(half, slots, kv.at[b, 0], kv.at[b, 1], qb, db, mb, gq_t, masked)
        return [(0, 0, grad_k[0]), (0, HEAD_DIM, grad_k[1]), (1, 0, grad_v)]

    def hold(at, pieces, add):
        for part, col, piece in pieces:
            cols = pl.ds(col, piece.shape[1])
            if add:
                acc[at, part, :, cols] += piece
            else:
                acc[at, part, :, cols] = piece

    def partial(b):
        return remote(p_out.at[b], p_in.at[b], p_send.at[b], p_recv.at[b], me, pair)

    def emit(b, pieces):
        for part, col, piece in pieces:
            cols = pl.ds(col, piece.shape[1])
            lo, hi = piece[:hrows], piece[hrows:]
            keep[b, part, :, cols] = jnp.where(c == 0, lo, hi)
            p_out[b, part, :, cols] = jnp.where(c == 0, hi, lo).astype(jnp.bfloat16)
        partial(b).start()

    def held(at):
        return [(part, 0, acc[at, part]) for part in range(2)]

    carried = jnp.where(home, c, 2)

    def down(b, part):
        return remote(dn_out.at[b, part], up_in.at[b, part], dn_send.at[b, part], up_recv.at[b, part], me - 2)

    def gk_hop(b, sems, target):
        return remote(gkb.at[b, carried], gkb.at[b, carried], sems.at[b], gk_recv.at[b, carried], target)

    def gk_give(b, sems, target, to):
        return remote(gkb.at[b, carried], gkb.at[b, c], sems.at[b], gk_recv.at[b, c], target, to)

    def gk_deliver(b, act):
        act(gk_give(b, gk_cross, mate, 2 * x + y))

        @pl.when(~home)
        def _():
            act(gk_give(b, gk_pair, me, pair))

    def gk_up_hop(b, act):
        @pl.when(has_up)
        def _():
            act(gk_hop(b, gk_up, me + 2))

    def gk_dn_hop(b, act):
        @pl.when(o > 0)
        def _():
            act(gk_hop(b, gk_dn, me - 2))

    def start(copy):
        copy.start()

    def gv_give(s):
        return remote(gv_fin.at[s], gv_in.at[c], gv_send.at[s], gv_recv.at[c], 2 * o + s, 2 * x + y)

    def each_of(level, act):
        @pl.loop(0, 2)
        def _(j):
            act(2 * level + jnp.where(j == 0, y, 1 - y))

    def reduce(b):
        landed(p_in.at[b], p_recv.at[b])
        for part in range(2):
            @pl.when(has_up)
            def _():
                landed(up_in.at[b, part], up_recv.at[b, part])
                keep[b, part] += up_in[b, part].astype(jnp.float32)

            total = keep[b, part] + p_in[b, part].astype(jnp.float32)

            @pl.when(b // 2 < o)
            def _():
                dn_out[b, part] = total.astype(jnp.bfloat16)
                down(b, part).start()

            @pl.when(b // 2 == o)
            def _():
                if part == 0:
                    gkb[b, carried] = (total * SCALE).astype(jnp.bfloat16)
                    gk_up_hop(b, start)
                    gk_dn_hop(b, start)
                    gk_deliver(b, start)
                else:
                    s = b % 2

                    @pl.when(home & (s == y))
                    def _():
                        gv_in[c] = total.astype(jnp.bfloat16)

                    @pl.when(~(home & (s == y)))
                    def _():
                        gv_fin[s] = total.astype(jnp.bfloat16)
                        gv_give(s).start()

    @pl.when(~home)
    def _():
        kv_wait(me, c)
        pass_up(me)
        rows_arrive(y)
        kv_wait(me, 1 - c)

    hold(y, grads(me, [y], True), False)
    take(mate)

    @pl.when(o > 0)
    def _():
        @pl.loop(0, 2)
        def _(j):
            b = 2 * (o - 1) + jnp.where(j == 0, y, 1 - y)
            take(b)
            kv_wait(b, 1 - c)
            hold(2 + b % 2, grads(b, [y]), False)

    kv_wait(mate, 1 - c)
    rows_arrive(1 - y)
    hold(1 - y, grads(mate, [1 - y], True), False)
    hold(0, grads(2 * o, [1]), True)
    emit(2 * o, held(0))
    emit(2 * o + 1, held(1))

    @pl.when(o > 0)
    def _():
        @pl.loop(0, 2)
        def _(j):
            b = 2 * (o - 1) + jnp.where(j == 0, y, 1 - y)
            hold(2 + b % 2, grads(b, [1 - y]), True)
            emit(b, held(2 + b % 2))

            @pl.when((j == 0) & ~has_up)
            def _():
                each_of(o, reduce)

    @pl.loop(2, o + 1)
    def _(t):
        @pl.loop(0, 2)
        def _(j):
            b = 2 * (o - t) + jnp.where(j == 0, y, 1 - y)
            take(b)
            kv_wait(b, 1 - c)
            emit(b, grads(b, [0, 1]))

            @pl.when((j == 0) & ~has_up)
            def _():
                each_of(o - t + 1, reduce)

    @pl.when(~has_up)
    def _():
        each_of(0, reduce)

    hid_late()

    def gq_give(s):
        return remote(gq_fin.at[s], gq_in.at[c], gq_send.at[s], gq_recv.at[c], 2 * o + s, 2 * x + y)

    @pl.loop(0, 2)
    def _(k):
        s = jnp.where(k == 0, 1 - y, y)
        local = home & (s == y)
        for at in range(2 * half):
            cols = slice(at * HEAD_DIM, (at + 1) * HEAD_DIM)
            piece = (gq_t[s, cols, :] * SCALE).T.astype(jnp.bfloat16)

            @pl.when(local)
            def _():
                gq_in[c, :, cols] = piece

            @pl.when(~local)
            def _():
                gq_fin[s, :, cols] = piece

        @pl.when(~local)
        def _():
            gq_give(s).start()

    @pl.when(has_up)
    def _():
        each_of(o, reduce)

    @pl.loop(o + 1, outer)
    def _(l):
        def step(b):
            landed(gkb.at[b, carried], gk_recv.at[b, carried])
            gk_dn_hop(b, start)
            gk_deliver(b, start)

        each_of(l, step)

    hid_wait(hid_recv.at[tp])

    @pl.loop(1, tp_count // 2)
    def _(k):
        hid_over(k).start()

    hid_to_pair(0).start()

    @pl.when(has_up)
    def _():
        @pl.loop(0, o)
        def _(k):
            each_of(o - 1 - k, reduce)

    @pl.loop(1, tp_count // 2)
    def _(k):
        source = (tp + 2 * k) % tp_count
        landed(hid.at[source], hid_recv.at[source])
        hid_to_pair(k).start()

    @pl.loop(0, tp_count // 2)
    def _(k):
        source = (pair + 2 * k) % tp_count
        landed(hid.at[source], hid_recv.at[source])

    def gk_ready(b):
        for h in range(2):
            @pl.when(~(home & (c == h)))
            def _():
                landed(gkb.at[b, h], gk_recv.at[b, h])

    def add_weight(b):
        gk_ready(b)
        block = jnp.concatenate([hid[k, b] for k in range(tp_count)], axis=0)
        gw_out[...] += dot_tn(block, jnp.concatenate([gkb[b, 0], gkb[b, 1]], axis=0))

    @pl.loop(0, outer)
    def _(k):
        l = jnp.where(k < outer - o, o + k, outer - 1 - k)

        @pl.when(l < o)
        def _():
            def step(b):
                landed(gkb.at[b, carried], gk_recv.at[b, carried])
                gk_up_hop(b, start)
                gk_deliver(b, start)

            each_of(l, step)

        each_of(l, add_weight)

    gk_out[:hrows] = gkb[me, 0]
    gk_out[hrows:] = gkb[me, 1]
    for h in range(2):
        @pl.when(~(home & (c == h)))
        def _():
            landed(gv_in.at[h], gv_recv.at[h])
            landed(gq_in.at[h], gq_recv.at[h])

        gv_out[h * hrows : (h + 1) * hrows] = gv_in[h]
        gq_out[:, h * pair_q : (h + 1) * pair_q] = gq_in[h]

    for p in range(2):
        own_copy(p).wait_send()

        @pl.when(not_self(p))
        def _():
            spread(qb, p, q_send, q_recv).wait_send()
            spread(db, p, d_send, d_recv).wait_send()
            spread(mb, p, m_send, m_recv).wait_send()

        @pl.when(~(home & (y == p)))
        def _():
            gv_give(p).wait_send()
            gq_give(p).wait_send()

    @pl.loop(0, 2 * o + 2)
    def _(b):
        @pl.when(has_up)
        def _():
            up_copy(b).wait_send()

        @pl.when(b != me)
        def _():
            pair_copy(b).wait_send()

        partial(b).wait_send()

        @pl.when(b // 2 < o)
        def _():
            for part in range(2):
                down(b, part).wait_send()

    @pl.loop(0, n)
    def _(b):
        @pl.when(b // 2 <= o)
        def _():
            gk_up_hop(b, lambda copy: copy.wait_send())

        @pl.when(b // 2 >= o)
        def _():
            gk_dn_hop(b, lambda copy: copy.wait_send())

        gk_deliver(b, lambda copy: copy.wait_send())

    hid_wait(hid_send)

    @pl.loop(1, tp_count // 2)
    def _(k):
        hid_over(k).wait_send()

    @pl.loop(0, tp_count // 2)
    def _(k):
        hid_to_pair(k).wait_send()


def write_kernel(*refs):
    for src, dst in zip(refs[:4], refs[4:]):
        dst[...] = src[...]


def on_device(n, tp_count, hidden, key_weight, queries, values, map_out, log_sums, out_grad, mixing, out_gain):
    rows = queries.shape[0]
    heads = mixing.shape[0]
    width = values.shape[1]
    half = heads // 2
    hrows = rows // 2
    assert width == V_DIM and n % 2 == 0 and tp_count % 2 == 0 and n >= 4
    bf16, f32 = jnp.bfloat16, jnp.float32
    vm = pl.BlockSpec(memory_space=VMEM)
    hbm = pl.BlockSpec(memory_space=pl.ANY)
    buffers = [
        VMEM(hidden.shape, bf16),
        VMEM(key_weight.shape, bf16),
        VMEM(map_out.shape, bf16),
        VMEM(out_grad.shape, bf16),
        VMEM((4, rows, half * 2 * HEAD_DIM), bf16),
        VMEM((4, rows, half * V_DIM), bf16),
        VMEM((4, 4 * half, rows), f32),
        VMEM((n + 1, 2, rows, width), bf16),
        VMEM((4, 2, rows, width), f32),
        VMEM((n, 2, hrows, width), f32),
        VMEM((n, 2, hrows, width), bf16),
        VMEM((n, 2, hrows, width), bf16),
        VMEM((n, 2, hrows, width), bf16),
        VMEM((n, 2, hrows, width), bf16),
        VMEM((n, 3, hrows, width), bf16),
        VMEM((2, hrows, width), bf16),
        VMEM((2, hrows, width), bf16),
        VMEM((2, half * 2 * HEAD_DIM, rows), f32),
        VMEM((2, rows, half * 2 * HEAD_DIM), bf16),
        VMEM((2, rows, half * 2 * HEAD_DIM), bf16),
        VMEM((tp_count, n, rows // tp_count, hidden.shape[1] // n), bf16),
    ]
    sems = [
        DMA((7,)),
        *[DMA((2,))] * 6,
        DMA((n, 2)),
        DMA((2,)),
        DMA((n,)),
        DMA((n,)),
        DMA((n,)),
        DMA((n,)),
        DMA((n, 2)),
        DMA((n, 2)),
        DMA((n, 3)),
        *[DMA((n,))] * 4,
        *[DMA((2,))] * 4,
        DMA,
        *[DMA((tp_count,))] * 3,
    ]
    results = pl.pallas_call(
        functools.partial(attend_kernel, n, tp_count, heads),
        out_shape=(
            jax.ShapeDtypeStruct(queries.shape, bf16),
            jax.ShapeDtypeStruct((rows, width), bf16),
            jax.ShapeDtypeStruct((rows, width), bf16),
            jax.ShapeDtypeStruct((hidden.shape[1] // n, width), f32),
        ),
        in_specs=[hbm] * 6 + [vm] * 2 + [pl.BlockSpec(memory_space=pltpu.SMEM)],
        out_specs=(vm, vm, vm, vm),
        scratch_shapes=buffers + sems,
        compiler_params=pltpu.CompilerParams(
            vmem_limit_bytes=60 * 2**20, collective_id=0, has_side_effects=True
        ),
        cost_estimate=pl.CostEstimate(flops=5 * 10**9, bytes_accessed=10**7, transcendentals=0),
    )(hidden, key_weight, values, queries, map_out, out_grad, log_sums, out_gain.reshape(1, V_DIM), mixing)
    return pl.pallas_call(
        write_kernel,
        out_shape=tuple(jax.ShapeDtypeStruct(r.shape, r.dtype) for r in results),
        in_specs=[vm] * 4,
        out_specs=(vm,) * 4,
        cost_estimate=pl.CostEstimate(flops=10**6, bytes_accessed=4 * 10**6, transcendentals=0),
    )(*results)


def solution(mesh):
    placed = (
        P("sp", None),
        P(None, "tp"),
        P("sp", "tp"),
        P("sp", "tp"),
        P("sp", "tp"),
        P("tp", "sp"),
        P("sp", "tp"),
        P("tp"),
        P(),
    )
    return jax.shard_map(
        functools.partial(on_device, mesh.shape["sp"], mesh.shape["tp"]),
        mesh=mesh,
        in_specs=placed,
        out_specs=(P("sp", "tp"), P("sp", "tp"), P("sp", "tp"), P("sp", "tp")),
        check_vma=False,
    )
```

```python
import functools
import math

import jax
import jax.numpy as jnp
from jax import lax
from jax.experimental import pallas as pl
from jax.experimental.pallas import tpu as pltpu
from jax.sharding import PartitionSpec as P

HEAD_DIM = 128
V_DIM = 256
OUT_SCALE = 0.8
NORM_EPS = 1e-06
LOG2E = math.log2(math.e)
SCALE = HEAD_DIM ** (-0.5)
VMEM = pltpu.VMEM
DMA = pltpu.SemaphoreType.DMA


def dot_nn(a, b):
    return lax.dot_general(a, b, (((1,), (0,)), ((), ())), preferred_element_type=jnp.float32)


def dot_nt(a, b):
    return lax.dot_general(a, b, (((1,), (1,)), ((), ())), preferred_element_type=jnp.float32)


def dot_tn(a, b):
    return lax.dot_general(a, b, (((0,), (0,)), ((), ())), preferred_element_type=jnp.float32)


def head_terms(pair, half, slot, og_ref, mo_ref, log_ref, mix_ref, gain_ref, d_ref, m_ref):
    gain = gain_ref[...] * OUT_SCALE
    rows = og_ref.shape[0]
    cols, lifts = [], []
    for i in range(half):
        h = pair * half + i
        at = pl.multiple_of(2 * h * V_DIM, V_DIM)
        map_a = mo_ref[:, pl.ds(at, V_DIM)].astype(jnp.float32)
        map_b = mo_ref[:, pl.ds(at + V_DIM, V_DIM)].astype(jnp.float32)
        pre = map_a - mix_ref[h] * map_b
        inv = lax.rsqrt(jnp.mean(pre * pre, axis=-1, keepdims=True) + NORM_EPS)
        up = og_ref[:, pl.ds(pl.multiple_of(h * V_DIM, V_DIM), V_DIM)].astype(jnp.float32) * gain
        d_out = inv * (up - pre * (inv * inv * jnp.mean(up * pre, axis=-1, keepdims=True)))
        d_ref[slot, :, i * V_DIM : (i + 1) * V_DIM] = d_out.astype(jnp.bfloat16)
        cols.append(jnp.sum(d_out * map_a, axis=-1, keepdims=True))
        cols.append(jnp.sum(d_out * map_b, axis=-1, keepdims=True))
        lifts.append(jnp.zeros((1, rows), jnp.float32))
        lifts.append(jnp.log(jnp.full((1, rows), mix_ref[h], jnp.float32)))
    lane = lax.broadcasted_iota(jnp.int32, (rows, 128), 1)
    packed = jnp.zeros((rows, 128), jnp.float32)
    for at, col in enumerate(cols):
        packed = jnp.where(lane == at, col, packed)
    logs = log_ref[...]
    logs = jnp.where(pair == 0, logs[: 2 * half], logs[2 * half :])
    m_ref[slot, : 2 * half] = (logs - jnp.concatenate(lifts, axis=0)) * LOG2E
    m_ref[slot, 2 * half :] = packed.T[: 2 * half]


def block_grads(half, slots, k_ref, v_ref, q_ref, d_ref, m_ref, gq_ref, masked):
    keys = [k_ref[:, m * HEAD_DIM : (m + 1) * HEAD_DIM] for m in range(2)]
    keys_t = [k.T for k in keys]
    vals = v_ref[...]
    grad_k = [None, None]
    grad_v = None
    for slot in slots:
        for i in range(half):
            d_h = d_ref[slot, :, i * V_DIM : (i + 1) * V_DIM]
            d_attn = dot_nt(vals, d_h)
            qs, probs, terms = [], [], []
            for m in range(2):
                at = 2 * i + m
                q = q_ref[slot, :, at * HEAD_DIM : (at + 1) * HEAD_DIM]
                p = jnp.exp2(dot_nt(keys[m], q) * (SCALE * LOG2E) - m_ref[slot, at : at + 1, :])
                if masked:
                    k_at = lax.broadcasted_iota(jnp.int32, p.shape, 0)
                    q_at = lax.broadcasted_iota(jnp.int32, p.shape, 1)
                    p = jnp.where(k_at <= q_at, p, 0.0)
                qs.append(q)
                probs.append(p)
                terms.append(m_ref[slot, 2 * half + at : 2 * half + at + 1, :])
            w = (probs[0] - probs[1]).astype(jnp.bfloat16)
            ds = [
                (probs[0] * (d_attn - terms[0])).astype(jnp.bfloat16),
                (probs[1] * (terms[1] - d_attn)).astype(jnp.bfloat16),
            ]
            for m in range(2):
                at = 2 * i + m
                gq_ref[slot, at * HEAD_DIM : (at + 1) * HEAD_DIM, :] += dot_nn(keys_t[m], ds[m])
                gk = dot_nn(ds[m], qs[m])
                grad_k[m] = gk if grad_k[m] is None else grad_k[m] + gk
            gv = dot_nn(w, d_h)
            grad_v = gv if grad_v is None else grad_v + gv
    return grad_k, grad_v


def attend_kernel(
    n, tp_count, heads,
    hidden_ref, weight_ref, values_ref, q_in_ref, mo_in_ref, og_in_ref, log_ref, gain_ref, mix_ref,
    gq_out, gk_out, gv_out, gw_out,
    hid_vm, w_vm, mo_vm, og_vm, qb, db, mb, kv, acc, keep, p_out, p_in, up_in, dn_out,
    gkb, gv_fin, gv_in, gq_t, gq_fin, gq_in, hid,
    load_sem, q_send, q_recv, d_send, d_recv, m_send, m_recv,
    kv_recv, kv_own, kv_up, kv_pair, p_send, p_recv, dn_send, up_recv,
    gk_recv, gk_up, gk_dn, gk_pair, gk_cross, gv_send, gv_recv, gq_send, gq_recv,
    hid_send, hid_src, hid_recv, hid_pass, hid_pair,
):
    me = lax.axis_index("sp")
    tp = lax.axis_index("tp")
    outer = n // 2
    half = heads // 2
    o, y = me // 2, me % 2
    x, c = tp // 2, tp % 2
    mate, pair = me + 1 - 2 * y, tp + 1 - 2 * c
    has_up = o < outer - 1
    home = y == c
    rows = og_in_ref.shape[0]
    hrows = rows // 2
    pair_q, pair_v = half * 2 * HEAD_DIM, half * V_DIM

    def remote(src, dst, send, recv, sp=me, to=tp):
        return pltpu.make_async_remote_copy(
            src_ref=src, dst_ref=dst, send_sem=send, recv_sem=recv, device_id={"sp": sp, "tp": to}
        )

    def landed(ref, sem):
        pltpu.make_async_copy(ref, ref, sem).wait()

    own_kv = jnp.where(home, me, n)

    def slot_of(p):
        return jnp.where(home & (p == c), y, 2 + p)

    def load(k):
        if k < 2:
            return pltpu.make_async_copy(
                q_in_ref.at[:, pl.ds(k * pair_q, pair_q)], qb.at[slot_of(k)], load_sem.at[k]
            )
        src, dst = {
            2: (values_ref, kv.at[own_kv, 1]),
            3: (hidden_ref, hid_vm),
            4: (weight_ref, w_vm),
            5: (mo_in_ref, mo_vm),
            6: (og_in_ref, og_vm),
        }[k]
        return pltpu.make_async_copy(src, dst, load_sem.at[k])

    for k in (2, 0, 1, 3, 4, 5, 6):
        load(k).start()

    barrier = pltpu.get_barrier_semaphore()

    @pl.loop(1, n)
    def _(k):
        pl.semaphore_signal(barrier, inc=1, device_id={"sp": (me + k) % n})

    @pl.loop(1, tp_count)
    def _(k):
        pl.semaphore_signal(barrier, inc=1, device_id={"tp": (tp + k) % tp_count})

    pl.semaphore_signal(barrier, inc=1, device_id={"sp": mate, "tp": pair})
    pl.semaphore_wait(barrier, n + tp_count - 1)

    def spread(buf, p, send, recv):
        return remote(buf.at[2 + p], buf.at[y], send.at[p], recv.at[y], 2 * o + c, 2 * x + p)

    def not_self(p):
        return ~(home & (p == c))

    def arrive(buf, slot, recv):
        landed(buf.at[slot], recv.at[slot])

    def rows_arrive(slot):
        arrive(qb, slot, q_recv)
        arrive(db, slot, d_recv)
        arrive(mb, slot, m_recv)

    def own_copy(p):
        return remote(
            kv.at[own_kv, p], kv.at[me, p], kv_own.at[p], kv_recv.at[me, p],
            2 * o + c, 2 * x + jnp.where(home, 1 - c, p),
        )

    def up_copy(b):
        return remote(kv.at[b, c], kv.at[b, c], kv_up.at[b], kv_recv.at[b, c], me + 2)

    def pair_copy(b):
        return remote(kv.at[b, c], kv.at[b, c], kv_pair.at[b], kv_recv.at[b, c], me, pair)

    def kv_wait(b, p):
        landed(kv.at[b, p], kv_recv.at[b, p])

    def pass_up(b):
        @pl.when(has_up)
        def _():
            up_copy(b).start()

    def take(b):
        kv_wait(b, c)
        pass_up(b)
        pair_copy(b).start()

    part_rows = rows // tp_count
    wide = hid_vm.shape[1] // n
    own_rows = pl.ds(pl.multiple_of(tp * part_rows, part_rows), part_rows)

    def columns(dest):
        return pl.ds(pl.multiple_of(dest * wide, wide), wide)

    def hid_slice(dest):
        return remote(hid_vm.at[own_rows, columns(dest)], hid.at[tp, me], hid_send, hid_src.at[me], dest)

    def hid_down(first, last, side):
        @pl.loop(first, last)
        def _(l):
            hid_slice(2 * l + side).start()

    def hid_over(k, b):
        block = hid.at[tp, b]
        return remote(block, block, hid_pass.at[k], hid_recv.at[tp], me, (tp + 2 * k) % tp_count)

    def hid_cross(first, last, side):
        @pl.loop(first, last)
        def _(l):
            b = 2 * l + side

            @pl.when(b != me)
            def _():
                landed(hid.at[tp, b], hid_src.at[b])

            @pl.loop(1, tp_count // 2)
            def _(k):
                hid_over(k, b).start()

    def hid_to_pair(k):
        source = (tp + 2 * k) % tp_count
        return remote(hid.at[source], hid.at[source], hid_pair.at[k], hid_recv.at[source], me, pair)

    defer = ~home & ~has_up
    load(2).wait()

    @pl.when(~defer)
    def _():
        own_copy(1).start()

    @pl.when(home & (c == 1) & has_up)
    def _():
        up_copy(me).start()

    def send_q(p):
        load(p).wait()

        @pl.when(not_self(p))
        def _():
            spread(qb, p, q_send, q_recv).start()

    @pl.when(~has_up)
    def _():
        send_q(0)
        send_q(1)

    load(3).wait()
    load(4).wait()
    kv[own_kv, 0] = dot_nn(hid_vm[...], w_vm[...]).astype(jnp.bfloat16)

    @pl.when(~defer)
    def _():
        own_copy(0).start()

    @pl.when(home & (c == 0) & has_up)
    def _():
        up_copy(me).start()

    @pl.when(has_up)
    def _():
        send_q(0)
        send_q(1)

    load(5).wait()
    load(6).wait()

    @pl.loop(0, 2)
    def _(k):
        p = jnp.where(k == 0, 1 - c, c)
        head_terms(p, half, slot_of(p), og_vm, mo_vm, log_ref, mix_ref, gain_ref, db, mb)

        @pl.when(not_self(p))
        def _():
            spread(db, p, d_send, d_recv).start()
            spread(mb, p, m_send, m_recv).start()

    @pl.when(defer)
    def _():
        own_copy(1).start()
        own_copy(0).start()

    hid[tp, me] = hid_vm[own_rows, columns(me)]
    hid_down(0, o, y)

    @pl.when(~home)
    def _():
        hid_down(0, o + 1, 1 - y)

    gw_out[...] = jnp.zeros_like(gw_out)
    gq_t[...] = jnp.zeros_like(gq_t)

    def grads(b, slots, masked=False):
        grad_k, grad_v = block_grads(half, slots, kv.at[b, 0], kv.at[b, 1], qb, db, mb, gq_t, masked)
        return [(0, 0, grad_k[0]), (0, HEAD_DIM, grad_k[1]), (1, 0, grad_v)]

    def hold(at, pieces, add):
        for part, col, piece in pieces:
            cols = pl.ds(col, piece.shape[1])
            if add:
                acc[at, part, :, cols] += piece
            else:
                acc[at, part, :, cols] = piece

    def partial(b):
        return remote(p_out.at[b], p_in.at[b], p_send.at[b], p_recv.at[b], me, pair)

    def emit(b, pieces):
        for part, col, piece in pieces:
            cols = pl.ds(col, piece.shape[1])
            lo, hi = piece[:hrows], piece[hrows:]
            keep[b, part, :, cols] = jnp.where(c == 0, lo, hi)
            p_out[b, part, :, cols] = jnp.where(c == 0, hi, lo).astype(jnp.bfloat16)
        partial(b).start()

    def held(at):
        return [(part, 0, acc[at, part]) for part in range(2)]

    carried = jnp.where(home, c, 2)

    def down(b, part):
        return remote(dn_out.at[b, part], up_in.at[b, part], dn_send.at[b, part], up_recv.at[b, part], me - 2)

    def gk_hop(b, sems, target):
        return remote(gkb.at[b, carried], gkb.at[b, carried], sems.at[b], gk_recv.at[b, carried], target)

    def gk_give(b, sems, target, to):
        return remote(gkb.at[b, carried], gkb.at[b, c], sems.at[b], gk_recv.at[b, c], target, to)

    def gk_deliver(b, act):
        act(gk_give(b, gk_cross, mate, 2 * x + y))

        @pl.when(~home)
        def _():
            act(gk_give(b, gk_pair, me, pair))

    def gk_up_hop(b, act):
        @pl.when(has_up)
        def _():
            act(gk_hop(b, gk_up, me + 2))

    def gk_dn_hop(b, act):
        @pl.when(o > 0)
        def _():
            act(gk_hop(b, gk_dn, me - 2))

    def start(copy):
        copy.start()

    def gv_give(s):
        return remote(gv_fin.at[s], gv_in.at[c], gv_send.at[s], gv_recv.at[c], 2 * o + s, 2 * x + y)

    def each_of(level, act):
        @pl.loop(0, 2)
        def _(j):
            act(2 * level + jnp.where(j == 0, y, 1 - y))

    def reduce(b):
        landed(p_in.at[b], p_recv.at[b])
        for part in range(2):
            @pl.when(has_up)
            def _():
                landed(up_in.at[b, part], up_recv.at[b, part])
                keep[b, part] += up_in[b, part].astype(jnp.float32)

            total = keep[b, part] + p_in[b, part].astype(jnp.float32)

            @pl.when(b // 2 < o)
            def _():
                dn_out[b, part] = total.astype(jnp.bfloat16)
                down(b, part).start()

            @pl.when(b // 2 == o)
            def _():
                if part == 0:
                    gkb[b, carried] = (total * SCALE).astype(jnp.bfloat16)
                    gk_up_hop(b, start)

                    gk_dn_hop(b, start)
                    gk_deliver(b, start)
                else:
                    s = b % 2

                    @pl.when(home & (s == y))
                    def _():
                        gv_in[c] = total.astype(jnp.bfloat16)

                    @pl.when(~(home & (s == y)))
                    def _():
                        gv_fin[s] = total.astype(jnp.bfloat16)
                        gv_give(s).start()

    @pl.when(~home)
    def _():
        kv_wait(me, c)
        pass_up(me)
        rows_arrive(y)
        kv_wait(me, 1 - c)

    hold(y, grads(me, [y], True), False)

    @pl.when(has_up)
    def _():
        take(mate)

    count = 2 * o

    def lower(i):
        return 2 * (o - 1 - i // 2) + jnp.where(i % 2 == 0, y, 1 - y)

    def take_lower(i):
        @pl.when(i < count)
        def _():
            take(lower(i))

    def top_reduce(i):
        @pl.when(~has_up)
        def _():
            reduce(lower(i))

    @pl.loop(0, jnp.minimum(count, 2))
    def _(i):
        b = lower(i)
        take(b)
        kv_wait(b, 1 - c)
        hold(2 + i, grads(b, [y]), False)

    take_lower(2)
    rows_arrive(1 - y)

    @pl.when(home)
    def _():
        hid_down(0, o + 1, 1 - y)

    @pl.loop(0, jnp.minimum(count, 2))
    def _(i):
        b = lower(i)
        hold(2 + i, grads(b, [1 - y]), True)
        emit(b, held(2 + i))

        @pl.when(i == 0)
        def _():
            take_lower(3)

            @pl.when(~has_up)
            def _():
                take(mate)

        @pl.when(i == 1)
        def _():
            top_reduce(0)

    @pl.loop(2, count)
    def _(i):
        b = lower(i)
        kv_wait(b, 1 - c)
        emit(b, grads(b, [0, 1]))
        take_lower(i + 2)
        top_reduce(i - 1)

    kv_wait(mate, 1 - c)
    hold(1 - y, grads(mate, [1 - y], True), False)
    top_reduce(count - 1)
    hold(0, grads(2 * o, [1]), True)
    emit(2 * o, held(0))
    emit(2 * o + 1, held(1))
    hid_down(o + 1, outer, y)
    hid_down(o + 1, outer, 1 - y)

    def gq_give(s):
        return remote(gq_fin.at[s], gq_in.at[c], gq_send.at[s], gq_recv.at[c], 2 * o + s, 2 * x + y)

    @pl.loop(0, 2)
    def _(k):
        s = jnp.where(k == 0, 1 - y, y)
        local = home & (s == y)
        for at in range(2 * half):
            cols = slice(at * HEAD_DIM, (at + 1) * HEAD_DIM)
            piece = (gq_t[s, cols, :] * SCALE).T.astype(jnp.bfloat16)

            @pl.when(local)
            def _():
                gq_in[c, :, cols] = piece

            @pl.when(~local)
            def _():
                gq_fin[s, :, cols] = piece

        @pl.when(~local)
        def _():
            gq_give(s).start()

    near_top = o >= outer - 2

    def hid_relay():
        hid_to_pair(0).start()

        @pl.loop(1, tp_count // 2)
        def _(k):
            source = (tp + 2 * k) % tp_count
            landed(hid.at[source], hid_recv.at[source])
            hid_to_pair(k).start()

    def hid_below():
        hid_cross(0, o, y)
        hid_cross(0, o, 1 - y)

    hid_cross(o, outer, y)
    hid_cross(o, outer, 1 - y)

    @pl.when(~near_top)
    def _():
        hid_below()

    def gk_step(b):
        landed(gkb.at[b, carried], gk_recv.at[b, carried])

        @pl.when(b // 2 < o)
        def _():
            gk_up_hop(b, start)

        @pl.when(b // 2 > o)
        def _():
            gk_dn_hop(b, start)

        gk_deliver(b, start)

    def gk_ready(b):
        for h in range(2):
            @pl.when(~(home & (c == h)))
            def _():
                landed(gkb.at[b, h], gk_recv.at[b, h])

    def add_weight(b):
        gk_ready(b)
        block = jnp.concatenate([hid[k, b] for k in range(tp_count)], axis=0)
        gw_out[...] += dot_tn(block, jnp.concatenate([gkb[b, 0], gkb[b, 1]], axis=0))

    def hid_finish():
        @pl.loop(0, tp_count // 2)
        def _(k):
            source = (pair + 2 * k) % tp_count
            landed(hid.at[source], hid_recv.at[source])

    first_up = jnp.where(near_top, o + 1, o + 2)

    @pl.when(o == 0)
    def _():
        hid_relay()

        @pl.loop(1, outer - 1)
        def _(l):
            each_of(l, gk_step)

        hid_finish()

        @pl.loop(1, outer - 1)
        def _(l):
            each_of(l, add_weight)

    @pl.when((o > 0) & ~near_top)
    def _():
        each_of(o + 1, gk_step)

    each_of(o, reduce)

    @pl.when(near_top)
    def _():
        hid_below()

    @pl.when(has_up)
    def _():
        @pl.loop(0, o)
        def _(k):
            each_of(o - 1 - k, reduce)

    @pl.when(o == 1)
    def _():
        each_of(0, gk_step)

    @pl.loop(jnp.where(o == 0, outer - 1, first_up), outer)
    def _(l):
        each_of(l, gk_step)

    @pl.when(o > 1)
    def _():
        each_of(o - 1, gk_step)

    @pl.when(o > 0)
    def _():
        hid_relay()
        hid_finish()

    @pl.loop(0, outer)
    def _(k):
        l = jnp.where(k < outer - o, o + k, outer - 1 - k)

        @pl.when(l < o - 1)
        def _():
            each_of(l, gk_step)

        @pl.when((o > 0) | (l == 0) | (l == outer - 1))
        def _():
            each_of(l, add_weight)

    gk_out[:hrows] = gkb[me, 0]
    gk_out[hrows:] = gkb[me, 1]
    for h in range(2):
        @pl.when(~(home & (c == h)))
        def _():
            landed(gv_in.at[h], gv_recv.at[h])
            landed(gq_in.at[h], gq_recv.at[h])

        gv_out[h * hrows : (h + 1) * hrows] = gv_in[h]
        gq_out[:, h * pair_q : (h + 1) * pair_q] = gq_in[h]

    for p in range(2):
        own_copy(p).wait_send()

        @pl.when(not_self(p))
        def _():
            spread(qb, p, q_send, q_recv).wait_send()
            spread(db, p, d_send, d_recv).wait_send()
            spread(mb, p, m_send, m_recv).wait_send()

        @pl.when(~(home & (y == p)))
        def _():
            gv_give(p).wait_send()
            gq_give(p).wait_send()

    @pl.loop(0, 2 * o + 2)
    def _(b):
        @pl.when(has_up)
        def _():
            up_copy(b).wait_send()

        @pl.when(b != me)
        def _():
            pair_copy(b).wait_send()

        partial(b).wait_send()

        @pl.when(b // 2 < o)
        def _():
            for part in range(2):
                down(b, part).wait_send()

    @pl.loop(0, n)
    def _(b):
        @pl.when(b // 2 <= o)
        def _():
            gk_up_hop(b, lambda copy: copy.wait_send())

        @pl.when(b // 2 >= o)
        def _():
            gk_dn_hop(b, lambda copy: copy.wait_send())

        gk_deliver(b, lambda copy: copy.wait_send())

    pieces = hid.at[tp, pl.ds(0, n - 1)]
    landed(pieces, hid_send)

    @pl.loop(1, tp_count // 2)
    def _(k):
        landed(hid.at[tp], hid_pass.at[k])

    @pl.loop(0, tp_count // 2)
    def _(k):
        hid_to_pair(k).wait_send()


def write_kernel(*refs):
    for src, dst in zip(refs[:4], refs[4:]):
        dst[...] = src[...]


def on_device(n, tp_count, hidden, key_weight, queries, values, map_out, log_sums, out_grad, mixing, out_gain):
    rows = queries.shape[0]
    heads = mixing.shape[0]
    width = values.shape[1]
    half = heads // 2
    hrows = rows // 2
    assert width == V_DIM and n % 2 == 0 and tp_count % 2 == 0 and n >= 4
    bf16, f32 = jnp.bfloat16, jnp.float32
    vm = pl.BlockSpec(memory_space=VMEM)
    hbm = pl.BlockSpec(memory_space=pl.ANY)
    buffers = [
        VMEM(hidden.shape, bf16),
        VMEM(key_weight.shape, bf16),
        VMEM(map_out.shape, bf16),
        VMEM(out_grad.shape, bf16),
        VMEM((4, rows, half * 2 * HEAD_DIM), bf16),
        VMEM((4, rows, half * V_DIM), bf16),
        VMEM((4, 4 * half, rows), f32),
        VMEM((n + 1, 2, rows, width), bf16),
        VMEM((4, 2, rows, width), f32),
        VMEM((n, 2, hrows, width), f32),
        VMEM((n, 2, hrows, width), bf16),
        VMEM((n, 2, hrows, width), bf16),
        VMEM((n, 2, hrows, width), bf16),
        VMEM((n, 2, hrows, width), bf16),
        VMEM((n, 3, hrows, width), bf16),
        VMEM((2, hrows, width), bf16),
        VMEM((2, hrows, width), bf16),
        VMEM((2, half * 2 * HEAD_DIM, rows), f32),
        VMEM((2, rows, half * 2 * HEAD_DIM), bf16),
        VMEM((2, rows, half * 2 * HEAD_DIM), bf16),
        VMEM((tp_count, n, rows // tp_count, hidden.shape[1] // n), bf16),
    ]
    sems = [
        DMA((7,)),
        *[DMA((2,))] * 6,
        DMA((n, 2)),
        DMA((2,)),
        DMA((n,)),
        DMA((n,)),
        DMA((n,)),
        DMA((n,)),
        DMA((n, 2)),
        DMA((n, 2)),
        DMA((n, 3)),
        *[DMA((n,))] * 4,
        *[DMA((2,))] * 4,
        DMA,
        DMA((n,)),
        *[DMA((tp_count,))] * 3,
    ]
    results = pl.pallas_call(
        functools.partial(attend_kernel, n, tp_count, heads),
        out_shape=(
            jax.ShapeDtypeStruct(queries.shape, bf16),
            jax.ShapeDtypeStruct((rows, width), bf16),
            jax.ShapeDtypeStruct((rows, width), bf16),
            jax.ShapeDtypeStruct((hidden.shape[1] // n, width), f32),
        ),
        in_specs=[hbm] * 6 + [vm] * 2 + [pl.BlockSpec(memory_space=pltpu.SMEM)],
        out_specs=(vm, vm, vm, vm),
        scratch_shapes=buffers + sems,
        compiler_params=pltpu.CompilerParams(
            vmem_limit_bytes=60 * 2**20, collective_id=0, has_side_effects=True
        ),
        cost_estimate=pl.CostEstimate(flops=5 * 10**9, bytes_accessed=10**7, transcendentals=0),
    )(hidden, key_weight, values, queries, map_out, out_grad, log_sums, out_gain.reshape(1, V_DIM), mixing)
    return pl.pallas_call(
        write_kernel,
        out_shape=tuple(jax.ShapeDtypeStruct(r.shape, r.dtype) for r in results),
        in_specs=[vm] * 4,
        out_specs=(vm,) * 4,
        cost_estimate=pl.CostEstimate(flops=10**6, bytes_accessed=4 * 10**6, transcendentals=0),
    )(*results)


def solution(mesh):
    placed = (
        P("sp", None),
        P(None, "tp"),
        P("sp", "tp"),
        P("sp", "tp"),
        P("sp", "tp"),
        P("tp", "sp"),
        P("sp", "tp"),
        P("tp"),
        P(),
    )
    return jax.shard_map(
        functools.partial(on_device, mesh.shape["sp"], mesh.shape["tp"]),
        mesh=mesh,
        in_specs=placed,
        out_specs=(P("sp", "tp"), P("sp", "tp"), P("sp", "tp"), P("sp", "tp")),
        check_vma=False,
    )
```

```python
import functools
import math

import jax
import jax.numpy as jnp
from jax import lax
from jax.experimental import pallas as pl
from jax.experimental.pallas import tpu as pltpu
from jax.sharding import PartitionSpec as P

HEAD_DIM = 128
V_DIM = 256
OUT_SCALE = 0.8
NORM_EPS = 1e-06
LOG2E = math.log2(math.e)
SCALE = HEAD_DIM ** (-0.5)
VMEM = pltpu.VMEM
DMA = pltpu.SemaphoreType.DMA


def dot_nn(a, b):
    return lax.dot_general(a, b, (((1,), (0,)), ((), ())), preferred_element_type=jnp.float32)


def dot_nt(a, b):
    return lax.dot_general(a, b, (((1,), (1,)), ((), ())), preferred_element_type=jnp.float32)


def dot_tn(a, b):
    return lax.dot_general(a, b, (((0,), (0,)), ((), ())), preferred_element_type=jnp.float32)


def head_terms(pair, half, slot, og_ref, mo_ref, log_ref, mix_ref, gain_ref, d_ref, m_ref):
    gain = gain_ref[...] * OUT_SCALE
    rows = og_ref.shape[0]
    cols, lifts = [], []
    for i in range(half):
        h = pair * half + i
        at = pl.multiple_of(2 * h * V_DIM, V_DIM)
        map_a = mo_ref[:, pl.ds(at, V_DIM)].astype(jnp.float32)
        map_b = mo_ref[:, pl.ds(at + V_DIM, V_DIM)].astype(jnp.float32)
        pre = map_a - mix_ref[h] * map_b
        inv = lax.rsqrt(jnp.mean(pre * pre, axis=-1, keepdims=True) + NORM_EPS)
        up = og_ref[:, pl.ds(pl.multiple_of(h * V_DIM, V_DIM), V_DIM)].astype(jnp.float32) * gain
        d_out = inv * (up - pre * (inv * inv * jnp.mean(up * pre, axis=-1, keepdims=True)))
        d_ref[slot, :, i * V_DIM : (i + 1) * V_DIM] = d_out.astype(jnp.bfloat16)
        cols.append(jnp.sum(d_out * map_a, axis=-1, keepdims=True))
        cols.append(jnp.sum(d_out * map_b, axis=-1, keepdims=True))
        lifts.append(jnp.zeros((1, rows), jnp.float32))
        lifts.append(jnp.log(jnp.full((1, rows), mix_ref[h], jnp.float32)))
    lane = lax.broadcasted_iota(jnp.int32, (rows, 128), 1)
    packed = jnp.zeros((rows, 128), jnp.float32)
    for at, col in enumerate(cols):
        packed = jnp.where(lane == at, col, packed)
    logs = log_ref[...]
    logs = jnp.where(pair == 0, logs[: 2 * half], logs[2 * half :])
    m_ref[slot, : 2 * half] = (logs - jnp.concatenate(lifts, axis=0)) * LOG2E
    m_ref[slot, 2 * half :] = packed.T[: 2 * half]


def block_grads(half, slots, k_ref, v_ref, q_ref, d_ref, m_ref, gq_ref, masked):
    keys = [k_ref[:, m * HEAD_DIM : (m + 1) * HEAD_DIM] for m in range(2)]
    keys_t = [k.T for k in keys]
    vals = v_ref[...]
    grad_k = [None, None]
    grad_v = None
    for slot in slots:
        for i in range(half):
            d_h = d_ref[slot, :, i * V_DIM : (i + 1) * V_DIM]
            d_attn = dot_nt(vals, d_h)
            qs, probs, terms = [], [], []
            for m in range(2):
                at = 2 * i + m
                q = q_ref[slot, :, at * HEAD_DIM : (at + 1) * HEAD_DIM]
                p = jnp.exp2(dot_nt(keys[m], q) * (SCALE * LOG2E) - m_ref[slot, at : at + 1, :])
                if masked:
                    k_at = lax.broadcasted_iota(jnp.int32, p.shape, 0)
                    q_at = lax.broadcasted_iota(jnp.int32, p.shape, 1)
                    p = jnp.where(k_at <= q_at, p, 0.0)
                qs.append(q)
                probs.append(p)
                terms.append(m_ref[slot, 2 * half + at : 2 * half + at + 1, :])
            w = (probs[0] - probs[1]).astype(jnp.bfloat16)
            ds = [
                (probs[0] * (d_attn - terms[0])).astype(jnp.bfloat16),
                (probs[1] * (terms[1] - d_attn)).astype(jnp.bfloat16),
            ]
            for m in range(2):
                at = 2 * i + m
                gq_ref[slot, at * HEAD_DIM : (at + 1) * HEAD_DIM, :] += dot_nn(keys_t[m], ds[m])
                gk = dot_nn(ds[m], qs[m])
                grad_k[m] = gk if grad_k[m] is None else grad_k[m] + gk
            gv = dot_nn(w, d_h)
            grad_v = gv if grad_v is None else grad_v + gv
    return grad_k, grad_v


def attend_kernel(
    n, tp_count, heads,
    hidden_ref, weight_ref, values_ref, q_in_ref, mo_in_ref, og_in_ref, log_ref, gain_ref, mix_ref,
    gq_out, gk_out, gv_out, gw_out,
    hid_vm, w_vm, mo_vm, og_vm, qb, db, mb, kv, acc, keep, p_out, p_in, up_in, dn_out,
    gkb, gv_fin, gv_in, gq_t, gq_fin, gq_in, hid,
    load_sem, q_send, q_recv, d_send, d_recv, m_send, m_recv,
    kv_recv, kv_own, kv_up, kv_pair, p_send, p_recv, dn_send, up_recv,
    gk_recv, gk_up, gk_dn, gk_pair, gk_cross, gv_send, gv_recv, gq_send, gq_recv,
    hid_send, hid_src, hid_recv, hid_pass, hid_pair,
):
    me = lax.axis_index("sp")
    tp = lax.axis_index("tp")
    outer = n // 2
    half = heads // 2
    o, y = me // 2, me % 2
    x, c = tp // 2, tp % 2
    mate, pair = me + 1 - 2 * y, tp + 1 - 2 * c
    has_up = o < outer - 1
    near_top = o >= outer - 2
    home = y == c
    rows = og_in_ref.shape[0]
    hrows = rows // 2
    pair_q, pair_v = half * 2 * HEAD_DIM, half * V_DIM

    def remote(src, dst, send, recv, sp=me, to=tp):
        return pltpu.make_async_remote_copy(
            src_ref=src, dst_ref=dst, send_sem=send, recv_sem=recv, device_id={"sp": sp, "tp": to}
        )

    def landed(ref, sem):
        pltpu.make_async_copy(ref, ref, sem).wait()

    own_kv = jnp.where(home, me, n)

    def slot_of(p):
        return jnp.where(home & (p == c), y, 2 + p)

    def load(k):
        if k < 2:
            return pltpu.make_async_copy(
                q_in_ref.at[:, pl.ds(k * pair_q, pair_q)], qb.at[slot_of(k)], load_sem.at[k]
            )
        src, dst = {
            2: (values_ref, kv.at[own_kv, 1]),
            3: (hidden_ref, hid_vm),
            4: (weight_ref, w_vm),
            5: (mo_in_ref, mo_vm),
            6: (og_in_ref, og_vm),
        }[k]
        return pltpu.make_async_copy(src, dst, load_sem.at[k])

    for k in (2, 0, 1, 3, 4, 5, 6):
        load(k).start()

    barrier = pltpu.get_barrier_semaphore()

    @pl.loop(1, n)
    def _(k):
        pl.semaphore_signal(barrier, inc=1, device_id={"sp": (me + k) % n})

    @pl.loop(1, tp_count)
    def _(k):
        pl.semaphore_signal(barrier, inc=1, device_id={"tp": (tp + k) % tp_count})

    pl.semaphore_signal(barrier, inc=1, device_id={"sp": mate, "tp": pair})
    pl.semaphore_wait(barrier, n + tp_count - 1)

    def spread(buf, p, send, recv):
        return remote(buf.at[2 + p], buf.at[y], send.at[p], recv.at[y], 2 * o + c, 2 * x + p)

    def not_self(p):
        return ~(home & (p == c))

    def arrive(buf, slot, recv):
        landed(buf.at[slot], recv.at[slot])

    def rows_arrive(slot):
        arrive(qb, slot, q_recv)
        arrive(db, slot, d_recv)
        arrive(mb, slot, m_recv)

    def own_copy(p):
        return remote(
            kv.at[own_kv, p], kv.at[me, p], kv_own.at[p], kv_recv.at[me, p],
            2 * o + c, 2 * x + jnp.where(home, 1 - c, p),
        )

    def up_copy(b):
        return remote(kv.at[b, c], kv.at[b, c], kv_up, kv_recv.at[b, c], me + 2)

    def pair_copy(b):
        return remote(kv.at[b, c], kv.at[b, c], kv_pair, kv_recv.at[b, c], me, pair)

    def kv_wait(b, p):
        landed(kv.at[b, p], kv_recv.at[b, p])

    def pass_up(b):
        @pl.when(has_up)
        def _():
            up_copy(b).start()

    def take(b):
        kv_wait(b, c)
        pass_up(b)
        pair_copy(b).start()

    part_rows = rows // tp_count
    wide = hid_vm.shape[1] // n
    own_rows = pl.ds(pl.multiple_of(tp * part_rows, part_rows), part_rows)

    def columns(dest):
        return pl.ds(pl.multiple_of(dest * wide, wide), wide)

    def hid_slice(dest):
        return remote(hid_vm.at[own_rows, columns(dest)], hid.at[tp, me], hid_send, hid_src.at[me], dest)

    def hid_down(first, last, side):
        @pl.loop(first, last)
        def _(l):
            hid_slice(2 * l + side).start()

    def hid_over(k, b):
        block = hid.at[tp, b]
        return remote(block, block, hid_pass.at[k], hid_recv.at[tp], me, (tp + 2 * k) % tp_count)

    def hid_cross(first, last, side):
        @pl.loop(first, last)
        def _(l):
            b = 2 * l + side

            @pl.when(b != me)
            def _():
                landed(hid.at[tp, b], hid_src.at[b])

            @pl.loop(1, tp_count // 2)
            def _(k):
                hid_over(k, b).start()

    def hid_to_pair(k):
        source = (tp + 2 * k) % tp_count
        return remote(hid.at[source], hid.at[source], hid_pair.at[k], hid_recv.at[source], me, pair)

    defer = ~home & ~has_up
    load(2).wait()

    @pl.when(~defer)
    def _():
        own_copy(1).start()

    @pl.when(home & (c == 1) & has_up)
    def _():
        up_copy(me).start()

    def send_q(p):
        load(p).wait()

        @pl.when(not_self(p))
        def _():
            spread(qb, p, q_send, q_recv).start()

    @pl.when(~has_up)
    def _():
        send_q(0)
        send_q(1)

    load(3).wait()
    load(4).wait()
    kv[own_kv, 0] = dot_nn(hid_vm[...], w_vm[...]).astype(jnp.bfloat16)

    @pl.when(~defer)
    def _():
        own_copy(0).start()

    @pl.when(home & (c == 0) & has_up)
    def _():
        up_copy(me).start()

    @pl.when(has_up)
    def _():
        send_q(0)
        send_q(1)

    load(5).wait()
    load(6).wait()

    @pl.loop(0, 2)
    def _(k):
        p = jnp.where(k == 0, 1 - c, c)
        head_terms(p, half, slot_of(p), og_vm, mo_vm, log_ref, mix_ref, gain_ref, db, mb)

        @pl.when(not_self(p))
        def _():
            spread(db, p, d_send, d_recv).start()
            spread(mb, p, m_send, m_recv).start()

    @pl.when(defer)
    def _():
        own_copy(1).start()
        own_copy(0).start()

    hid[tp, me] = hid_vm[own_rows, columns(me)]
    hid_down(0, o, y)

    @pl.when(~home)
    def _():
        hid_down(0, o + 1, 1 - y)

    gw_out[...] = jnp.zeros_like(gw_out)
    gq_t[...] = jnp.zeros_like(gq_t)

    def grads(b, slots, masked=False):
        grad_k, grad_v = block_grads(half, slots, kv.at[b, 0], kv.at[b, 1], qb, db, mb, gq_t, masked)
        return [(0, 0, grad_k[0]), (0, HEAD_DIM, grad_k[1]), (1, 0, grad_v)]

    def hold(at, pieces, add):
        for part, col, piece in pieces:
            cols = pl.ds(col, piece.shape[1])
            if add:
                acc[at, part, :, cols] += piece
            else:
                acc[at, part, :, cols] = piece

    def partial(b):
        return remote(p_out.at[b], p_in.at[b], p_send, p_recv.at[b], me, pair)

    def emit(b, pieces):
        for part, col, piece in pieces:
            cols = pl.ds(col, piece.shape[1])
            lo, hi = piece[:hrows], piece[hrows:]
            keep[b, part, :, cols] = jnp.where(c == 0, lo, hi)
            p_out[b, part, :, cols] = jnp.where(c == 0, hi, lo).astype(jnp.bfloat16)
        partial(b).start()

    def held(at):
        return [(part, 0, acc[at, part]) for part in range(2)]

    carried = jnp.where(home, c, 2)
    reach = 3

    def down(b, part):
        return remote(dn_out.at[b, part], up_in.at[b, part], dn_send, up_recv.at[b, part], me - 2)

    def gk_hop(b, sems, target):
        return remote(gkb.at[b, carried], gkb.at[b, carried], sems, gk_recv.at[b, 1], target)

    def gk_give(b, sems, target, to):
        return remote(gkb.at[b, carried], gkb.at[b, c], sems, gk_recv.at[b, 0], target, to)

    def gk_deliver(b, act):
        act(gk_give(b, gk_cross, mate, 2 * x + y))

        @pl.when(~home)
        def _():
            act(gk_give(b, gk_pair, me, pair))

    def gk_up_hop(b, act):
        @pl.when((o - b // 2) % reach == 0)
        def _():
            for k in range(reach, 0, -1):
                @pl.when(o + k < outer)
                def _():
                    act(gk_hop(b, gk_up, me + 2 * k))

    def gk_dn_hop(b, act):
        @pl.when(o > 0)
        def _():
            act(gk_hop(b, gk_dn, me - 2))

    def start(copy):
        copy.start()

    def gv_give(s):
        return remote(gv_fin.at[s], gv_in.at[c], gv_send.at[s], gv_recv.at[c], 2 * o + s, 2 * x + y)

    def each_of(level, act):
        @pl.loop(0, 2)
        def _(j):
            act(2 * level + jnp.where(j == 0, y, 1 - y))

    def reduce(b, part):
        if part == 0:
            landed(p_in.at[b], p_recv.at[b])

        @pl.when(has_up)
        def _():
            landed(up_in.at[b, part], up_recv.at[b, part])
            keep[b, part] += up_in[b, part].astype(jnp.float32)

        total = keep[b, part] + p_in[b, part].astype(jnp.float32)

        @pl.when(b // 2 < o)
        def _():
            dn_out[b, part] = total.astype(jnp.bfloat16)
            down(b, part).start()

        @pl.when(b // 2 == o)
        def _():
            if part == 0:
                gkb[b, carried] = (total * SCALE).astype(jnp.bfloat16)
                gk_up_hop(b, start)
                gk_dn_hop(b, start)
                gk_deliver(b, start)
            else:
                s = b % 2

                @pl.when(home & (s == y))
                def _():
                    gv_in[c] = total.astype(jnp.bfloat16)

                @pl.when(~(home & (s == y)))
                def _():
                    gv_fin[s] = total.astype(jnp.bfloat16)
                    gv_give(s).start()

    def sums(level, part):
        each_of(level, lambda b: reduce(b, part))

    @pl.when(~home)
    def _():
        kv_wait(me, c)
        pass_up(me)
        rows_arrive(y)
        kv_wait(me, 1 - c)

    hold(y, grads(me, [y], True), False)

    @pl.when(has_up)
    def _():
        take(mate)

    count = 2 * o

    def lower(i):
        return 2 * (o - 1 - i // 2) + jnp.where(i % 2 == 0, y, 1 - y)

    def take_lower(i):
        @pl.when(i < count)
        def _():
            take(lower(i))

    def top_reduce(i):
        @pl.when(~has_up)
        def _():
            reduce(lower(i), 0)

            @pl.when(i < 2)
            def _():
                reduce(lower(i), 1)

    @pl.loop(0, jnp.minimum(count, 2))
    def _(i):
        b = lower(i)
        take(b)
        kv_wait(b, 1 - c)
        hold(2 + i, grads(b, [y]), False)

    take_lower(2)

    @pl.when(has_up)
    def _():
        take_lower(3)

    rows_arrive(1 - y)

    @pl.when(home)
    def _():
        hid_down(0, o + 1, 1 - y)

    @pl.loop(0, jnp.minimum(count, 2))
    def _(i):
        b = lower(i)
        hold(2 + i, grads(b, [1 - y]), True)
        emit(b, held(2 + i))

        @pl.when((i == 0) & ~has_up)
        def _():
            take_lower(3)

        @pl.when(i == 1)
        def _():
            top_reduce(0)

    hid_down(o + 1, outer, y)
    hid_down(o + 1, outer, 1 - y)
    hid_cross(o, outer, y)

    @pl.loop(2, count)
    def _(i):
        b = lower(i)
        kv_wait(b, 1 - c)
        emit(b, grads(b, [0, 1]))
        take_lower(i + 2)
        top_reduce(i - 1)

    @pl.when(~has_up)
    def _():
        take(mate)
        hid_cross(o, outer, 1 - y)
        hid_cross(o - 1, o, y)
        hid_cross(o - 1, o, 1 - y)

    kv_wait(mate, 1 - c)
    hold(1 - y, grads(mate, [1 - y], True), False)
    top_reduce(count - 1)
    hold(0, grads(2 * o, [1]), True)
    emit(2 * o, held(0))
    emit(2 * o + 1, held(1))

    @pl.when(~has_up & (count > 2))
    def _():
        sums(0, 1)

    @pl.when(has_up & near_top)
    def _():
        hid_cross(o, outer, 1 - y)

    def gq_give(s):
        return remote(gq_fin.at[s], gq_in.at[c], gq_send.at[s], gq_recv.at[c], 2 * o + s, 2 * x + y)

    @pl.loop(0, 2)
    def _(k):
        s = jnp.where(k == 0, 1 - y, y)
        local = home & (s == y)
        for at in range(2 * half):
            cols = slice(at * HEAD_DIM, (at + 1) * HEAD_DIM)
            piece = (gq_t[s, cols, :] * SCALE).T.astype(jnp.bfloat16)

            @pl.when(local)
            def _():
                gq_in[c, :, cols] = piece

            @pl.when(~local)
            def _():
                gq_fin[s, :, cols] = piece

        @pl.when(~local)
        def _():
            gq_give(s).start()

    def hid_relay():
        hid_to_pair(0).start()

        @pl.loop(1, tp_count // 2)
        def _(k):
            source = (tp + 2 * k) % tp_count
            landed(hid.at[source], hid_recv.at[source])
            hid_to_pair(k).start()

    def hid_below(last):
        hid_cross(0, last, y)
        hid_cross(0, last, 1 - y)

    @pl.when(~near_top)
    def _():
        hid_cross(o, outer, 1 - y)
        hid_below(o)

    def gk_step(b):
        landed(gkb.at[b, carried], gk_recv.at[b, 1])

        @pl.when(b // 2 < o)
        def _():
            gk_up_hop(b, start)

        @pl.when(b // 2 > o)
        def _():
            gk_dn_hop(b, start)

        gk_deliver(b, start)

    def gk_ready(b):
        @pl.when(home)
        def _():
            landed(gkb.at[b, 0], gk_recv.at[b, 0])

        @pl.when(~home)
        def _():
            landed(gkb.at[b, pl.ds(0, 2)], gk_recv.at[b, 0])

    def add_weight(b):
        gk_ready(b)
        block = jnp.concatenate([hid[k, b] for k in range(tp_count)], axis=0)
        gw_out[...] += dot_tn(block, jnp.concatenate([gkb[b, 0], gkb[b, 1]], axis=0))

    def hid_finish():
        @pl.loop(0, tp_count // 2)
        def _(k):
            source = (pair + 2 * k) % tp_count
            landed(hid.at[source], hid_recv.at[source])

    def settle():
        for p in range(2):
            own_copy(p).wait_send()

            @pl.when(not_self(p))
            def _():
                spread(qb, p, q_send, q_recv).wait_send()
                spread(db, p, d_send, d_recv).wait_send()
                spread(mb, p, m_send, m_recv).wait_send()

            @pl.when(~(home & (y == p)))
            def _():
                gq_give(p).wait_send()

            @pl.when(~(home & (c == p)))
            def _():
                landed(gq_in.at[p], gq_recv.at[p])

            gq_out[:, p * pair_q : (p + 1) * pair_q] = gq_in[p]

        for l in range(outer):
            @pl.when(o == l)
            def _():
                if l < outer - 1:
                    landed(kv.at[pl.ds(0, 2 * l + 2), 0], kv_up)
                landed(kv.at[pl.ds(0, 2 * l + 1), 0], kv_pair)
                landed(p_out.at[pl.ds(0, 2 * l + 2)], p_send)

        landed(hid.at[tp, pl.ds(0, n - 1)], hid_send)

        @pl.loop(1, tp_count // 2)
        def _(k):
            landed(hid.at[tp], hid_pass.at[k])

    def finish():
        gk_out[:hrows] = gkb[me, 0]
        gk_out[hrows:] = gkb[me, 1]
        for h in range(2):
            @pl.when(~(home & (c == h)))
            def _():
                landed(gv_in.at[h], gv_recv.at[h])

            gv_out[h * hrows : (h + 1) * hrows] = gv_in[h]

            @pl.when(~(home & (y == h)))
            def _():
                gv_give(h).wait_send()

        for l in range(1, outer):
            @pl.when(o == l)
            def _():
                landed(dn_out.at[pl.ds(0, 2 * l)], dn_send)
                landed(gkb.at[pl.ds(0, n - 2 * l), 0], gk_dn)

        @pl.loop(0, tp_count // 2)
        def _(k):
            hid_to_pair(k).wait_send()

    first_up = jnp.where(near_top, o + 1, o + 2)

    @pl.when(o == 0)
    def _():
        hid_relay()

        @pl.loop(1, outer - 1)
        def _(l):
            each_of(l, gk_step)

        hid_finish()

        @pl.loop(1, outer - 1)
        def _(l):
            each_of(l, add_weight)

        settle()

    @pl.when((o > 0) & ~near_top)
    def _():
        each_of(o + 1, gk_step)

    sums(o, 0)

    @pl.when((o == outer - 2) | (o == 0))
    def _():
        sums(o, 1)

    @pl.when(near_top)
    def _():
        hid_below(jnp.where(has_up, o, o - 1))

    @pl.when(has_up & (o > 0))
    def _():
        @pl.loop(0, o)
        def _(k):
            sums(o - 1 - k, 0)

        sums(0, 1)

    @pl.loop(jnp.where(o == 0, outer - 1, first_up), outer)
    def _(l):
        each_of(l, gk_step)

    @pl.loop(1, jnp.where(has_up, o, o - 1))
    def _(l):
        sums(l, 1)

    @pl.when((o != outer - 2) & (o > 0))
    def _():
        sums(o, 1)

    @pl.loop(1, o)
    def _(k):
        each_of(o - k, gk_step)

    @pl.when(o > 0)
    def _():
        hid_relay()
        hid_finish()
        settle()
        each_of(0, gk_step)

    @pl.loop(0, outer)
    def _(k):
        l = jnp.where(k < outer - o, o + k, outer - 1 - k)

        @pl.when(k == outer - 1)
        def _():
            finish()

        @pl.when((o > 0) | (l == 0) | (l == outer - 1))
        def _():
            each_of(l, add_weight)

    for l in range(outer - 1):
        hops = 2 * min(reach, outer - 1 - l) * (l // reach + 1)

        @pl.when(o == l)
        def _():
            landed(gkb.at[pl.ds(0, hops), 0], gk_up)

    landed(gkb.at[pl.ds(0, n), 0], gk_cross)

    @pl.when(~home)
    def _():
        landed(gkb.at[pl.ds(0, n), 0], gk_pair)


def write_kernel(*refs):
    copies = [pltpu.make_async_copy(refs[k], refs[4 + k], refs[8].at[k]) for k in range(4)]
    for copy in copies:
        copy.start()
    for copy in copies:
        copy.wait()


def on_device(n, tp_count, hidden, key_weight, queries, values, map_out, log_sums, out_grad, mixing, out_gain):
    rows = queries.shape[0]
    heads = mixing.shape[0]
    width = values.shape[1]
    half = heads // 2
    hrows = rows // 2
    assert width == V_DIM and n % 2 == 0 and tp_count % 2 == 0 and n >= 4
    bf16, f32 = jnp.bfloat16, jnp.float32
    vm = pl.BlockSpec(memory_space=VMEM)
    hbm = pl.BlockSpec(memory_space=pl.ANY)
    buffers = [
        VMEM(hidden.shape, bf16),
        VMEM(key_weight.shape, bf16),
        VMEM(map_out.shape, bf16),
        VMEM(out_grad.shape, bf16),
        VMEM((4, rows, half * 2 * HEAD_DIM), bf16),
        VMEM((4, rows, half * V_DIM), bf16),
        VMEM((4, 4 * half, rows), f32),
        VMEM((n + 1, 2, rows, width), bf16),
        VMEM((4, 2, rows, width), f32),
        VMEM((n, 2, hrows, width), f32),
        VMEM((n, 2, hrows, width), bf16),
        VMEM((n, 2, hrows, width), bf16),
        VMEM((n, 2, hrows, width), bf16),
        VMEM((n, 2, hrows, width), bf16),
        VMEM((n, 3, hrows, width), bf16),
        VMEM((2, hrows, width), bf16),
        VMEM((2, hrows, width), bf16),
        VMEM((2, half * 2 * HEAD_DIM, rows), f32),
        VMEM((2, rows, half * 2 * HEAD_DIM), bf16),
        VMEM((2, rows, half * 2 * HEAD_DIM), bf16),
        VMEM((tp_count, n, rows // tp_count, hidden.shape[1] // n), bf16),
    ]
    sems = [
        DMA((7,)),
        *[DMA((2,))] * 6,
        DMA((n, 2)),
        DMA((2,)),
        *[DMA] * 3,
        DMA((n,)),
        DMA,
        DMA((n, 2)),
        DMA((n, 2)),
        *[DMA] * 4,
        *[DMA((2,))] * 4,
        DMA,
        DMA((n,)),
        DMA((tp_count,)),
        *[DMA((tp_count // 2,))] * 2,
    ]
    results = pl.pallas_call(
        functools.partial(attend_kernel, n, tp_count, heads),
        out_shape=(
            VMEM(queries.shape, bf16),
            VMEM((rows, width), bf16),
            VMEM((rows, width), bf16),
            VMEM((hidden.shape[1] // n, width), f32),
        ),
        in_specs=[hbm] * 6 + [vm] * 2 + [pl.BlockSpec(memory_space=pltpu.SMEM)],
        out_specs=(vm, vm, vm, vm),
        scratch_shapes=buffers + sems,
        compiler_params=pltpu.CompilerParams(
            vmem_limit_bytes=60 * 2**20, collective_id=0, has_side_effects=True
        ),
        cost_estimate=pl.CostEstimate(flops=5 * 10**9, bytes_accessed=10**7, transcendentals=0),
    )(hidden, key_weight, values, queries, map_out, out_grad, log_sums, out_gain.reshape(1, V_DIM), mixing)
    return pl.pallas_call(
        write_kernel,
        out_shape=tuple(jax.ShapeDtypeStruct(r.shape, r.dtype) for r in results),
        in_specs=[vm] * 4,
        out_specs=(hbm,) * 4,
        scratch_shapes=[DMA((4,))],
        cost_estimate=pl.CostEstimate(flops=10**6, bytes_accessed=4 * 10**6, transcendentals=0),
    )(*[pltpu.with_memory_space_constraint(r, VMEM) for r in results])


def solution(mesh):
    placed = (
        P("sp", None),
        P(None, "tp"),
        P("sp", "tp"),
        P("sp", "tp"),
        P("sp", "tp"),
        P("tp", "sp"),
        P("sp", "tp"),
        P("tp"),
        P(),
    )
    return jax.shard_map(
        functools.partial(on_device, mesh.shape["sp"], mesh.shape["tp"]),
        mesh=mesh,
        in_specs=placed,
        out_specs=(P("sp", "tp"), P("sp", "tp"), P("sp", "tp"), P("sp", "tp")),
        check_vma=False,
    )
```

```python
import functools
import math

import jax
import jax.numpy as jnp
from jax import lax
from jax.experimental import pallas as pl
from jax.experimental.pallas import tpu as pltpu
from jax.sharding import PartitionSpec as P

HEAD_DIM = 128
V_DIM = 256
OUT_SCALE = 0.8
NORM_EPS = 1e-06
LOG2E = math.log2(math.e)
SCALE = HEAD_DIM ** (-0.5)
VMEM = pltpu.VMEM
DMA = pltpu.SemaphoreType.DMA


def dot_nn(a, b):
    return lax.dot_general(a, b, (((1,), (0,)), ((), ())), preferred_element_type=jnp.float32)


def dot_nt(a, b):
    return lax.dot_general(a, b, (((1,), (1,)), ((), ())), preferred_element_type=jnp.float32)


def dot_tn(a, b):
    return lax.dot_general(a, b, (((0,), (0,)), ((), ())), preferred_element_type=jnp.float32)


def head_terms(pair, half, slot, og_ref, mo_ref, log_ref, mix_ref, gain_ref, d_ref, m_ref):
    gain = gain_ref[...] * OUT_SCALE
    rows = og_ref.shape[0]
    cols, lifts = [], []
    for i in range(half):
        h = pair * half + i
        at = pl.multiple_of(2 * h * V_DIM, V_DIM)
        map_a = mo_ref[:, pl.ds(at, V_DIM)].astype(jnp.float32)
        map_b = mo_ref[:, pl.ds(at + V_DIM, V_DIM)].astype(jnp.float32)
        pre = map_a - mix_ref[h] * map_b
        inv = lax.rsqrt(jnp.mean(pre * pre, axis=-1, keepdims=True) + NORM_EPS)
        up = og_ref[:, pl.ds(pl.multiple_of(h * V_DIM, V_DIM), V_DIM)].astype(jnp.float32) * gain
        d_out = inv * (up - pre * (inv * inv * jnp.mean(up * pre, axis=-1, keepdims=True)))
        d_ref[slot, :, i * V_DIM : (i + 1) * V_DIM] = d_out.astype(jnp.bfloat16)
        cols.append(jnp.sum(d_out * map_a, axis=-1, keepdims=True))
        cols.append(jnp.sum(d_out * map_b, axis=-1, keepdims=True))
        lifts.append(jnp.zeros((1, rows), jnp.float32))
        lifts.append(jnp.log(jnp.full((1, rows), mix_ref[h], jnp.float32)))
    lane = lax.broadcasted_iota(jnp.int32, (rows, 128), 1)
    packed = jnp.zeros((rows, 128), jnp.float32)
    for at, col in enumerate(cols):
        packed = jnp.where(lane == at, col, packed)
    logs = log_ref[...]
    logs = jnp.where(pair == 0, logs[: 2 * half], logs[2 * half :])
    m_ref[slot, : 2 * half] = (logs - jnp.concatenate(lifts, axis=0)) * LOG2E
    m_ref[slot, 2 * half :] = packed.T[: 2 * half]


def block_grads(half, slots, k_ref, v_ref, q_ref, d_ref, m_ref, gq_ref, masked):
    keys = [k_ref[:, m * HEAD_DIM : (m + 1) * HEAD_DIM] for m in range(2)]
    keys_t = [k.T for k in keys]
    vals = v_ref[...]
    grad_k = [None, None]
    grad_v = None
    for slot in slots:
        for i in range(half):
            d_h = d_ref[slot, :, i * V_DIM : (i + 1) * V_DIM]
            d_attn = dot_nt(vals, d_h)
            qs, probs, terms = [], [], []
            for m in range(2):
                at = 2 * i + m
                q = q_ref[slot, :, at * HEAD_DIM : (at + 1) * HEAD_DIM]
                p = jnp.exp2(dot_nt(keys[m], q) * (SCALE * LOG2E) - m_ref[slot, at : at + 1, :])
                if masked:
                    k_at = lax.broadcasted_iota(jnp.int32, p.shape, 0)
                    q_at = lax.broadcasted_iota(jnp.int32, p.shape, 1)
                    p = jnp.where(k_at <= q_at, p, 0.0)
                qs.append(q)
                probs.append(p)
                terms.append(m_ref[slot, 2 * half + at : 2 * half + at + 1, :])
            w = (probs[0] - probs[1]).astype(jnp.bfloat16)
            ds = [
                (probs[0] * (d_attn - terms[0])).astype(jnp.bfloat16),
                (probs[1] * (terms[1] - d_attn)).astype(jnp.bfloat16),
            ]
            for m in range(2):
                at = 2 * i + m
                gq_ref[slot, at * HEAD_DIM : (at + 1) * HEAD_DIM, :] += dot_nn(keys_t[m], ds[m])
                gk = dot_nn(ds[m], qs[m])
                grad_k[m] = gk if grad_k[m] is None else grad_k[m] + gk
            gv = dot_nn(w, d_h)
            grad_v = gv if grad_v is None else grad_v + gv
    return grad_k, grad_v


def attend_kernel(
    n, tp_count, heads,
    hidden_ref, weight_ref, values_ref, q_in_ref, mo_in_ref, og_in_ref, log_ref, gain_ref, mix_ref,
    gq_out, gk_out, gv_out, gw_out,
    hid_vm, w_vm, mo_vm, og_vm, qb, db, mb, kv, acc, keep, p_out, p_in, up_in, dn_out,
    gkb, gv_fin, gv_in, gq_t, gq_fin, gq_in, hid,
    load_sem, q_send, q_recv, d_send, d_recv, m_send, m_recv,
    kv_recv, kv_own, kv_up, kv_pair, p_send, p_recv, dn_send, up_recv,
    gk_recv, gk_up, gk_dn, gk_pair, gk_cross, gv_send, gv_recv, gq_send, gq_recv,
    hid_send, hid_src, hid_recv, hid_pass, hid_pair,
):
    me = lax.axis_index("sp")
    tp = lax.axis_index("tp")
    outer = n // 2
    half = heads // 2
    o, y = me // 2, me % 2
    x, c = tp // 2, tp % 2
    mate, pair = me + 1 - 2 * y, tp + 1 - 2 * c
    has_up = o < outer - 1
    near_top = o >= outer - 2
    home = y == c
    rows = og_in_ref.shape[0]
    hrows = rows // 2
    pair_q, pair_v = half * 2 * HEAD_DIM, half * V_DIM

    def remote(src, dst, send, recv, sp=me, to=tp):
        return pltpu.make_async_remote_copy(
            src_ref=src, dst_ref=dst, send_sem=send, recv_sem=recv, device_id={"sp": sp, "tp": to}
        )

    def landed(ref, sem):
        pltpu.make_async_copy(ref, ref, sem).wait()

    own_kv = jnp.where(home, me, n)

    def slot_of(p):
        return jnp.where(home & (p == c), y, 2 + p)

    def load(k):
        if k < 2:
            return pltpu.make_async_copy(
                q_in_ref.at[:, pl.ds(k * pair_q, pair_q)], qb.at[slot_of(k)], load_sem.at[k]
            )
        src, dst = {
            2: (values_ref, kv.at[own_kv, 1]),
            3: (hidden_ref, hid_vm),
            4: (weight_ref, w_vm),
            5: (mo_in_ref, mo_vm),
            6: (og_in_ref, og_vm),
        }[k]
        return pltpu.make_async_copy(src, dst, load_sem.at[k])

    for k in (2, 0, 1, 3, 4, 5, 6):
        load(k).start()

    barrier = pltpu.get_barrier_semaphore()

    @pl.loop(1, n)
    def _(k):
        pl.semaphore_signal(barrier, inc=1, device_id={"sp": (me + k) % n})

    @pl.loop(1, tp_count)
    def _(k):
        pl.semaphore_signal(barrier, inc=1, device_id={"tp": (tp + k) % tp_count})

    pl.semaphore_signal(barrier, inc=1, device_id={"sp": mate, "tp": pair})
    pl.semaphore_wait(barrier, n + tp_count - 1)

    def spread(buf, p, send, recv):
        return remote(buf.at[2 + p], buf.at[y], send.at[p], recv.at[y], 2 * o + c, 2 * x + p)

    def not_self(p):
        return ~(home & (p == c))

    def arrive(buf, slot, recv):
        landed(buf.at[slot], recv.at[slot])

    def rows_arrive(slot):
        arrive(qb, slot, q_recv)
        arrive(db, slot, d_recv)
        arrive(mb, slot, m_recv)

    def own_copy(p):
        return remote(
            kv.at[own_kv, p], kv.at[me, p], kv_own.at[p], kv_recv.at[me, p],
            2 * o + c, 2 * x + jnp.where(home, 1 - c, p),
        )

    def up_copy(b):
        return remote(kv.at[b, c], kv.at[b, c], kv_up, kv_recv.at[b, c], me + 2)

    def pair_copy(b):
        return remote(kv.at[b, c], kv.at[b, c], kv_pair, kv_recv.at[b, c], me, pair)

    def kv_wait(b, p):
        landed(kv.at[b, p], kv_recv.at[b, p])

    def pass_up(b):
        @pl.when(has_up)
        def _():
            up_copy(b).start()

    def take(b):
        kv_wait(b, c)
        pass_up(b)
        pair_copy(b).start()

    part_rows = rows // tp_count
    wide = hid_vm.shape[1] // n
    own_rows = pl.ds(pl.multiple_of(tp * part_rows, part_rows), part_rows)

    def columns(dest):
        return pl.ds(pl.multiple_of(dest * wide, wide), wide)

    def hid_slice(dest):
        return remote(hid_vm.at[own_rows, columns(dest)], hid.at[tp, me], hid_send, hid_src.at[me], dest)

    def hid_down(first, last, side):
        @pl.loop(first, last)
        def _(l):
            hid_slice(2 * l + side).start()

    def hid_over(k, b):
        block = hid.at[tp, b]
        return remote(block, block, hid_pass.at[k], hid_recv.at[tp], me, (tp + 2 * k) % tp_count)

    def hid_cross(first, last, side):
        @pl.loop(first, last)
        def _(l):
            b = 2 * l + side

            @pl.when(b != me)
            def _():
                landed(hid.at[tp, b], hid_src.at[b])

            @pl.loop(1, tp_count // 2)
            def _(k):
                hid_over(k, b).start()

    def hid_to_pair(k):
        source = (tp + 2 * k) % tp_count
        return remote(hid.at[source], hid.at[source], hid_pair.at[k], hid_recv.at[source], me, pair)

    defer = ~home & ~has_up
    load(2).wait()

    @pl.when(~defer)
    def _():
        own_copy(1).start()

    @pl.when(home & (c == 1) & has_up)
    def _():
        up_copy(me).start()

    def send_q(p):
        load(p).wait()

        @pl.when(not_self(p))
        def _():
            spread(qb, p, q_send, q_recv).start()

    @pl.when(~has_up)
    def _():
        send_q(0)
        send_q(1)

    load(3).wait()
    load(4).wait()
    kv[own_kv, 0] = dot_nn(hid_vm[...], w_vm[...]).astype(jnp.bfloat16)

    @pl.when(~defer)
    def _():
        own_copy(0).start()

    @pl.when(home & (c == 0) & has_up)
    def _():
        up_copy(me).start()

    @pl.when(has_up)
    def _():
        send_q(0)
        send_q(1)

    load(5).wait()
    load(6).wait()

    @pl.loop(0, 2)
    def _(k):
        p = jnp.where(k == 0, 1 - c, c)
        head_terms(p, half, slot_of(p), og_vm, mo_vm, log_ref, mix_ref, gain_ref, db, mb)

        @pl.when(not_self(p))
        def _():
            spread(db, p, d_send, d_recv).start()
            spread(mb, p, m_send, m_recv).start()

    @pl.when(defer)
    def _():
        own_copy(1).start()
        own_copy(0).start()

    hid[tp, me] = hid_vm[own_rows, columns(me)]
    hid_down(0, o, y)

    @pl.when(~home)
    def _():
        hid_down(0, o + 1, 1 - y)

    gw_out[...] = jnp.zeros_like(gw_out)
    gq_t[...] = jnp.zeros_like(gq_t)

    def grads(b, slots, masked=False):
        grad_k, grad_v = block_grads(half, slots, kv.at[b, 0], kv.at[b, 1], qb, db, mb, gq_t, masked)
        return [(0, 0, grad_k[0]), (0, HEAD_DIM, grad_k[1]), (1, 0, grad_v)]

    def hold(at, pieces, add):
        for part, col, piece in pieces:
            cols = pl.ds(col, piece.shape[1])
            if add:
                acc[at, part, :, cols] += piece
            else:
                acc[at, part, :, cols] = piece

    def partial(b):
        return remote(p_out.at[b], p_in.at[b], p_send, p_recv.at[b], me, pair)

    def emit(b, pieces):
        for part, col, piece in pieces:
            cols = pl.ds(col, piece.shape[1])
            lo, hi = piece[:hrows], piece[hrows:]
            keep[b, part, :, cols] = jnp.where(c == 0, lo, hi)
            p_out[b, part, :, cols] = jnp.where(c == 0, hi, lo).astype(jnp.bfloat16)
        partial(b).start()

    def held(at):
        return [(part, 0, acc[at, part]) for part in range(2)]

    carried = jnp.where(home, c, 2)
    reach = 3

    def down(b, part):
        return remote(dn_out.at[b, part], up_in.at[b, part], dn_send, up_recv.at[b, part], me - 2)

    def gk_hop(b, sems, target):
        return remote(gkb.at[b, carried], gkb.at[b, carried], sems, gk_recv.at[b, 1], target)

    def gk_give(b, sems, target, to):
        return remote(gkb.at[b, carried], gkb.at[b, c], sems, gk_recv.at[b, 0], target, to)

    def gk_deliver(b, act):
        act(gk_give(b, gk_cross, mate, 2 * x + y))

        @pl.when(~home)
        def _():
            act(gk_give(b, gk_pair, me, pair))

    def gk_up_near(b):
        dist = (o - b // 2) % reach

        @pl.when(has_up & ((dist == 0) | ((dist == 1) & (o + 2 < outer))))
        def _():
            gk_hop(b, gk_up, me + 2).start()

    def gk_up_far(b):
        root = (o - b // 2) % reach == 0

        @pl.when(root & (o + 3 < outer))
        def _():
            gk_hop(b, gk_up, me + 6).start()

        @pl.when(root & (o + 3 == outer))
        def _():
            gk_hop(b, gk_up, me + 4).start()

    def gk_dn_hop(b, act):
        @pl.when(o > 0)
        def _():
            act(gk_hop(b, gk_dn, me - 2))

    def start(copy):
        copy.start()

    def gv_give(s):
        return remote(gv_fin.at[s], gv_in.at[c], gv_send.at[s], gv_recv.at[c], 2 * o + s, 2 * x + y)

    def each_of(level, act):
        @pl.loop(0, 2)
        def _(j):
            act(2 * level + jnp.where(j == 0, y, 1 - y))

    def reduce(b, part):
        if part == 0:
            landed(p_in.at[b], p_recv.at[b])

        @pl.when(has_up)
        def _():
            landed(up_in.at[b, part], up_recv.at[b, part])
            keep[b, part] += up_in[b, part].astype(jnp.float32)

        total = keep[b, part] + p_in[b, part].astype(jnp.float32)

        @pl.when(b // 2 < o)
        def _():
            dn_out[b, part] = total.astype(jnp.bfloat16)
            down(b, part).start()

        @pl.when(b // 2 == o)
        def _():
            if part == 0:
                gkb[b, carried] = (total * SCALE).astype(jnp.bfloat16)
                gk_up_near(b)

                @pl.when(b % 2 != y)
                def _():
                    each_of(o, gk_up_far)

                gk_dn_hop(b, start)
                gk_deliver(b, start)
            else:
                s = b % 2

                @pl.when(home & (s == y))
                def _():
                    gv_in[c] = total.astype(jnp.bfloat16)

                @pl.when(~(home & (s == y)))
                def _():
                    gv_fin[s] = total.astype(jnp.bfloat16)
                    gv_give(s).start()

    def sums(level, part):
        each_of(level, lambda b: reduce(b, part))

    @pl.when(~home)
    def _():
        kv_wait(me, c)
        pass_up(me)
        rows_arrive(y)
        kv_wait(me, 1 - c)

    hold(y, grads(me, [y], True), False)

    @pl.when(has_up)
    def _():
        take(mate)

    count = 2 * o

    def lower(i):
        return 2 * (o - 1 - i // 2) + jnp.where(i % 2 == 0, y, 1 - y)

    def take_lower(i):
        @pl.when(i < count)
        def _():
            take(lower(i))

    def top_reduce(i):
        @pl.when(~has_up)
        def _():
            reduce(lower(i), 0)

            @pl.when(i == 1)
            def _():
                reduce(lower(0), 1)
                reduce(lower(1), 1)

    ahead = jnp.minimum(count, jnp.where(has_up, 4, 2))

    @pl.loop(0, ahead)
    def _(i):
        b = lower(i)
        take(b)
        kv_wait(b, 1 - c)
        hold(2 + i, grads(b, [y]), False)

    @pl.when(~has_up)
    def _():
        take_lower(2)

    rows_arrive(1 - y)

    @pl.when(home)
    def _():
        hid_down(0, o + 1, 1 - y)

    def own_level():
        kv_wait(mate, 1 - c)
        hold(1 - y, grads(mate, [1 - y], True), False)
        top_reduce(count - 1)
        hold(0, grads(2 * o, [1]), True)
        emit(2 * o, held(0))
        emit(2 * o + 1, held(1))

    def hid_up():
        hid_down(o + 1, outer, y)
        hid_down(o + 1, outer, 1 - y)

    @pl.when(o == 0)
    def _():
        hid_up()

    @pl.when(has_up)
    def _():
        own_level()

    @pl.when(o > 0)
    def _():
        hid_up()

    below_top = has_up & near_top

    @pl.loop(0, ahead)
    def _(i):
        b = lower(i)
        hold(2 + i, grads(b, [1 - y]), True)
        emit(b, held(2 + i))

        @pl.when(i == 1)
        def _():
            top_reduce(0)

            @pl.when(below_top)
            def _():
                sums(o, 0)

    hid_cross(o, outer, y)

    @pl.when(has_up)
    def _():
        take_lower(4)
        take_lower(5)

    @pl.loop(ahead, count)
    def _(i):
        b = lower(i)
        kv_wait(b, 1 - c)
        emit(b, grads(b, [0, 1]))
        top_reduce(i - 1)

        @pl.when((i == 2) & ~has_up)
        def _():
            take_lower(3)

        take_lower(i + 2)

        @pl.when((i == count - 2) & ~has_up)
        def _():
            take(mate)

    @pl.when(~has_up)
    def _():
        @pl.when(count == 2)
        def _():
            take(mate)

        own_level()

        @pl.when(count > 2)
        def _():
            sums(0, 1)

    def gq_give(s):
        return remote(gq_fin.at[s], gq_in.at[c], gq_send.at[s], gq_recv.at[c], 2 * o + s, 2 * x + y)

    @pl.loop(0, 2)
    def _(k):
        s = jnp.where(k == 0, 1 - y, y)
        local = home & (s == y)
        for at in range(2 * half):
            cols = slice(at * HEAD_DIM, (at + 1) * HEAD_DIM)
            piece = (gq_t[s, cols, :] * SCALE).T.astype(jnp.bfloat16)

            @pl.when(local)
            def _():
                gq_in[c, :, cols] = piece

            @pl.when(~local)
            def _():
                gq_fin[s, :, cols] = piece

        @pl.when(~local)
        def _():
            gq_give(s).start()

    def hid_relay():
        hid_to_pair(0).start()

        @pl.loop(1, tp_count // 2)
        def _(k):
            source = (tp + 2 * k) % tp_count
            landed(hid.at[source], hid_recv.at[source])
            hid_to_pair(k).start()

    def hid_below(last):
        hid_cross(0, last, y)
        hid_cross(0, last, 1 - y)

    @pl.when(~near_top)
    def _():
        hid_cross(o, outer, 1 - y)
        hid_below(o)

    def gk_step(b):
        landed(gkb.at[b, carried], gk_recv.at[b, 1])

        @pl.when(b // 2 < o)
        def _():
            gk_up_near(b)
            gk_up_far(b)

        @pl.when(b // 2 > o)
        def _():
            gk_dn_hop(b, start)

        gk_deliver(b, start)

    def gk_ready(b):
        @pl.when(home)
        def _():
            landed(gkb.at[b, 0], gk_recv.at[b, 0])

        @pl.when(~home)
        def _():
            landed(gkb.at[b, pl.ds(0, 2)], gk_recv.at[b, 0])

    def add_weight(b):
        gk_ready(b)
        block = jnp.concatenate([hid[k, b] for k in range(tp_count)], axis=0)
        gw_out[...] += dot_tn(block, jnp.concatenate([gkb[b, 0], gkb[b, 1]], axis=0))

    def hid_finish():
        @pl.loop(0, tp_count // 2)
        def _(k):
            source = (pair + 2 * k) % tp_count
            landed(hid.at[source], hid_recv.at[source])

    def settle():
        for p in range(2):
            own_copy(p).wait_send()

            @pl.when(not_self(p))
            def _():
                spread(qb, p, q_send, q_recv).wait_send()
                spread(db, p, d_send, d_recv).wait_send()
                spread(mb, p, m_send, m_recv).wait_send()

            @pl.when(~(home & (y == p)))
            def _():
                gq_give(p).wait_send()

            @pl.when(~(home & (c == p)))
            def _():
                landed(gq_in.at[p], gq_recv.at[p])

            gq_out[:, p * pair_q : (p + 1) * pair_q] = gq_in[p]

        for l in range(outer):
            @pl.when(o == l)
            def _():
                if l < outer - 1:
                    landed(kv.at[pl.ds(0, 2 * l + 2), 0], kv_up)
                landed(kv.at[pl.ds(0, 2 * l + 1), 0], kv_pair)
                landed(p_out.at[pl.ds(0, 2 * l + 2)], p_send)

        landed(hid.at[tp, pl.ds(0, n - 1)], hid_send)

        @pl.loop(1, tp_count // 2)
        def _(k):
            landed(hid.at[tp], hid_pass.at[k])

    def finish():
        gk_out[:hrows] = gkb[me, 0]
        gk_out[hrows:] = gkb[me, 1]
        for h in range(2):
            @pl.when(~(home & (c == h)))
            def _():
                landed(gv_in.at[h], gv_recv.at[h])

            gv_out[h * hrows : (h + 1) * hrows] = gv_in[h]

            @pl.when(~(home & (y == h)))
            def _():
                gv_give(h).wait_send()

        for l in range(1, outer):
            @pl.when(o == l)
            def _():
                landed(dn_out.at[pl.ds(0, 2 * l)], dn_send)
                landed(gkb.at[pl.ds(0, n - 2 * l), 0], gk_dn)

        @pl.loop(0, tp_count // 2)
        def _(k):
            hid_to_pair(k).wait_send()

    first_up = jnp.where(near_top, o + 1, o + 2)

    @pl.when(o == 0)
    def _():
        hid_relay()

        @pl.loop(1, outer - 1)
        def _(l):
            each_of(l, gk_step)

        hid_finish()
        settle()

    @pl.when((o > 0) & ~near_top)
    def _():
        each_of(o + 1, gk_step)

    @pl.when(~below_top)
    def _():
        sums(o, 0)

    @pl.when(~has_up)
    def _():
        hid_cross(o, outer, 1 - y)
        hid_cross(o - 1, o, y)
        hid_cross(o - 1, o, 1 - y)

    @pl.when(o == 0)
    def _():
        @pl.loop(1, outer - 1)
        def _(l):
            each_of(l, add_weight)

    @pl.when((o == outer - 2) | (o == 0))
    def _():
        sums(o, 1)

    @pl.when(has_up & (o > 0))
    def _():
        @pl.loop(0, o)
        def _(k):
            sums(o - 1 - k, 0)

            @pl.when(near_top & (k == 0))
            def _():
                hid_cross(o, outer, 1 - y)
                hid_below(o)

        sums(0, 1)

    @pl.when(~has_up)
    def _():
        hid_below(o - 1)

    @pl.when((o == 1) & has_up)
    def _():
        hid_relay()

    @pl.loop(jnp.where(o == 0, outer - 1, first_up), outer)
    def _(l):
        each_of(l, gk_step)

    @pl.when((o == 1) & has_up)
    def _():
        each_of(0, gk_step)

    @pl.loop(1, jnp.where(has_up, o, o - 1))
    def _(l):
        sums(l, 1)

    @pl.when((o != outer - 2) & (o > 0))
    def _():
        sums(o, 1)

    @pl.loop(1, o)
    def _(k):
        each_of(o - k, gk_step)

    @pl.when((o > 1) | ~has_up)
    def _():
        hid_relay()

    @pl.when(o > 0)
    def _():
        hid_finish()
        settle()

        @pl.loop(1, outer)
        def _(k):
            each_of(jnp.where(k < outer - o + 1, o + k - 1, outer - k), add_weight)

    @pl.when(o == 0)
    def _():
        each_of(0, add_weight)

    finish()

    @pl.when((o > 1) | ~has_up)
    def _():
        each_of(0, gk_step)

    each_of(jnp.where(o == 0, outer - 1, 0), add_weight)

    for l in range(outer - 1):
        roots, nexts = l // reach + 1, (l - 1) // reach + 1
        hops = 2 * roots * min(2, outer - 1 - l) + 2 * nexts * (l + 2 < outer)

        @pl.when(o == l)
        def _():
            landed(gkb.at[pl.ds(0, hops), 0], gk_up)

    landed(gkb.at[pl.ds(0, n), 0], gk_cross)

    @pl.when(~home)
    def _():
        landed(gkb.at[pl.ds(0, n), 0], gk_pair)


def write_kernel(*refs):
    copies = [pltpu.make_async_copy(refs[k], refs[4 + k], refs[8].at[k]) for k in range(4)]
    for copy in copies:
        copy.start()
    for copy in copies:
        copy.wait()


def on_device(n, tp_count, hidden, key_weight, queries, values, map_out, log_sums, out_grad, mixing, out_gain):
    rows = queries.shape[0]
    heads = mixing.shape[0]
    width = values.shape[1]
    half = heads // 2
    hrows = rows // 2
    assert width == V_DIM and n % 2 == 0 and tp_count % 2 == 0 and n >= 4
    bf16, f32 = jnp.bfloat16, jnp.float32
    vm = pl.BlockSpec(memory_space=VMEM)
    hbm = pl.BlockSpec(memory_space=pl.ANY)
    buffers = [
        VMEM(hidden.shape, bf16),
        VMEM(key_weight.shape, bf16),
        VMEM(map_out.shape, bf16),
        VMEM(out_grad.shape, bf16),
        VMEM((4, rows, half * 2 * HEAD_DIM), bf16),
        VMEM((4, rows, half * V_DIM), bf16),
        VMEM((4, 4 * half, rows), f32),
        VMEM((n + 1, 2, rows, width), bf16),
        VMEM((6, 2, rows, width), f32),
        VMEM((n, 2, hrows, width), f32),
        VMEM((n, 2, hrows, width), bf16),
        VMEM((n, 2, hrows, width), bf16),
        VMEM((n, 2, hrows, width), bf16),
        VMEM((n, 2, hrows, width), bf16),
        VMEM((n, 3, hrows, width), bf16),
        VMEM((2, hrows, width), bf16),
        VMEM((2, hrows, width), bf16),
        VMEM((2, half * 2 * HEAD_DIM, rows), f32),
        VMEM((2, rows, half * 2 * HEAD_DIM), bf16),
        VMEM((2, rows, half * 2 * HEAD_DIM), bf16),
        VMEM((tp_count, n, rows // tp_count, hidden.shape[1] // n), bf16),
    ]
    sems = [
        DMA((7,)),
        *[DMA((2,))] * 6,
        DMA((n, 2)),
        DMA((2,)),
        *[DMA] * 3,
        DMA((n,)),
        DMA,
        DMA((n, 2)),
        DMA((n, 2)),
        *[DMA] * 4,
        *[DMA((2,))] * 4,
        DMA,
        DMA((n,)),
        DMA((tp_count,)),
        *[DMA((tp_count // 2,))] * 2,
    ]
    results = pl.pallas_call(
        functools.partial(attend_kernel, n, tp_count, heads),
        out_shape=(
            VMEM(queries.shape, bf16),
            VMEM((rows, width), bf16),
            VMEM((rows, width), bf16),
            VMEM((hidden.shape[1] // n, width), f32),
        ),
        in_specs=[hbm] * 6 + [vm] * 2 + [pl.BlockSpec(memory_space=pltpu.SMEM)],
        out_specs=(vm, vm, vm, vm),
        scratch_shapes=buffers + sems,
        compiler_params=pltpu.CompilerParams(
            vmem_limit_bytes=60 * 2**20, collective_id=0, has_side_effects=True
        ),
        cost_estimate=pl.CostEstimate(flops=5 * 10**9, bytes_accessed=10**7, transcendentals=0),
    )(hidden, key_weight, values, queries, map_out, out_grad, log_sums, out_gain.reshape(1, V_DIM), mixing)
    return pl.pallas_call(
        write_kernel,
        out_shape=tuple(jax.ShapeDtypeStruct(r.shape, r.dtype) for r in results),
        in_specs=[vm] * 4,
        out_specs=(hbm,) * 4,
        scratch_shapes=[DMA((4,))],
        cost_estimate=pl.CostEstimate(flops=10**6, bytes_accessed=4 * 10**6, transcendentals=0),
    )(*[pltpu.with_memory_space_constraint(r, VMEM) for r in results])


def solution(mesh):
    placed = (
        P("sp", None),
        P(None, "tp"),
        P("sp", "tp"),
        P("sp", "tp"),
        P("sp", "tp"),
        P("tp", "sp"),
        P("sp", "tp"),
        P("tp"),
        P(),
    )
    return jax.shard_map(
        functools.partial(on_device, mesh.shape["sp"], mesh.shape["tp"]),
        mesh=mesh,
        in_specs=placed,
        out_specs=(P("sp", "tp"), P("sp", "tp"), P("sp", "tp"), P("sp", "tp")),
        check_vma=False,
    )
```

```python
import functools
import math

import jax
import jax.numpy as jnp
from jax import lax
from jax.experimental import pallas as pl
from jax.experimental.pallas import tpu as pltpu
from jax.sharding import PartitionSpec as P

HEAD_DIM = 128
V_DIM = 256
OUT_SCALE = 0.8
NORM_EPS = 1e-06
LOG2E = math.log2(math.e)
SCALE = HEAD_DIM ** (-0.5)
VMEM = pltpu.VMEM
DMA = pltpu.SemaphoreType.DMA


def dot_nn(a, b):
    return lax.dot_general(a, b, (((1,), (0,)), ((), ())), preferred_element_type=jnp.float32)


def dot_nt(a, b):
    return lax.dot_general(a, b, (((1,), (1,)), ((), ())), preferred_element_type=jnp.float32)


def dot_tn(a, b):
    return lax.dot_general(a, b, (((0,), (0,)), ((), ())), preferred_element_type=jnp.float32)


def head_terms(pair, half, slot, og_ref, mo_ref, log_ref, mix_ref, gain_ref, d_ref, m_ref):
    gain = gain_ref[...] * OUT_SCALE
    rows = og_ref.shape[0]
    cols, lifts = [], []
    for i in range(half):
        h = pair * half + i
        at = pl.multiple_of(2 * h * V_DIM, V_DIM)
        map_a = mo_ref[:, pl.ds(at, V_DIM)].astype(jnp.float32)
        map_b = mo_ref[:, pl.ds(at + V_DIM, V_DIM)].astype(jnp.float32)
        pre = map_a - mix_ref[h] * map_b
        inv = lax.rsqrt(jnp.mean(pre * pre, axis=-1, keepdims=True) + NORM_EPS)
        up = og_ref[:, pl.ds(pl.multiple_of(h * V_DIM, V_DIM), V_DIM)].astype(jnp.float32) * gain
        d_out = inv * (up - pre * (inv * inv * jnp.mean(up * pre, axis=-1, keepdims=True)))
        d_ref[slot, :, i * V_DIM : (i + 1) * V_DIM] = d_out.astype(jnp.bfloat16)
        cols.append(jnp.sum(d_out * map_a, axis=-1, keepdims=True))
        cols.append(jnp.sum(d_out * map_b, axis=-1, keepdims=True))
        lifts.append(jnp.zeros((1, rows), jnp.float32))
        lifts.append(jnp.log(jnp.full((1, rows), mix_ref[h], jnp.float32)))
    lane = lax.broadcasted_iota(jnp.int32, (rows, 128), 1)
    packed = jnp.zeros((rows, 128), jnp.float32)
    for at, col in enumerate(cols):
        packed = jnp.where(lane == at, col, packed)
    logs = log_ref[...]
    logs = jnp.where(pair == 0, logs[: 2 * half], logs[2 * half :])
    m_ref[slot, : 2 * half] = (logs - jnp.concatenate(lifts, axis=0)) * LOG2E
    m_ref[slot, 2 * half :] = packed.T[: 2 * half]


def block_grads(half, slots, k_ref, v_ref, q_ref, d_ref, m_ref, gq_ref, masked):
    keys = [k_ref[:, m * HEAD_DIM : (m + 1) * HEAD_DIM] for m in range(2)]
    keys_t = [k.T for k in keys]
    vals = v_ref[...]
    grad_k = [None, None]
    grad_v = None
    for slot in slots:
        for i in range(half):
            d_h = d_ref[slot, :, i * V_DIM : (i + 1) * V_DIM]
            d_attn = dot_nt(vals, d_h)
            qs, probs, terms = [], [], []
            for m in range(2):
                at = 2 * i + m
                q = q_ref[slot, :, at * HEAD_DIM : (at + 1) * HEAD_DIM]
                p = jnp.exp2(dot_nt(keys[m], q) * (SCALE * LOG2E) - m_ref[slot, at : at + 1, :])
                if masked:
                    k_at = lax.broadcasted_iota(jnp.int32, p.shape, 0)
                    q_at = lax.broadcasted_iota(jnp.int32, p.shape, 1)
                    p = jnp.where(k_at <= q_at, p, 0.0)
                qs.append(q)
                probs.append(p)
                terms.append(m_ref[slot, 2 * half + at : 2 * half + at + 1, :])
            w = (probs[0] - probs[1]).astype(jnp.bfloat16)
            ds = [
                (probs[0] * (d_attn - terms[0])).astype(jnp.bfloat16),
                (probs[1] * (terms[1] - d_attn)).astype(jnp.bfloat16),
            ]
            for m in range(2):
                at = 2 * i + m
                gq_ref[slot, at * HEAD_DIM : (at + 1) * HEAD_DIM, :] += dot_nn(keys_t[m], ds[m])
                gk = dot_nn(ds[m], qs[m])
                grad_k[m] = gk if grad_k[m] is None else grad_k[m] + gk
            gv = dot_nn(w, d_h)
            grad_v = gv if grad_v is None else grad_v + gv
    return grad_k, grad_v


def attend_kernel(
    n, tp_count, heads,
    hidden_ref, weight_ref, values_ref, q_in_ref, mo_in_ref, og_in_ref, log_ref, gain_ref, mix_ref,
    gq_out, gk_out, gv_out, gw_out,
    hid_vm, w_vm, mo_vm, og_vm, qb, db, mb, kv, acc, keep, p_out, p_in, up_in, dn_out,
    gkb, gv_fin, gv_in, gq_t, gq_fin, gq_in, hid,
    load_sem, q_send, q_recv, d_send, d_recv, m_send, m_recv,
    kv_recv, kv_own, kv_up, kv_pair, p_send, p_recv, dn_send, up_recv,
    gk_recv, gk_up, gk_dn, gk_pair, gk_cross, gv_send, gv_recv, gq_send, gq_recv,
    hid_send, hid_src, hid_recv, hid_pass, hid_pair,
):
    me = lax.axis_index("sp")
    tp = lax.axis_index("tp")
    outer = n // 2
    half = heads // 2
    o, y = me // 2, me % 2
    x, c = tp // 2, tp % 2
    mate, pair = me + 1 - 2 * y, tp + 1 - 2 * c
    has_up = o < outer - 1
    near_top = o >= outer - 2
    home = y == c
    rows = og_in_ref.shape[0]
    hrows = rows // 2
    pair_q, pair_v = half * 2 * HEAD_DIM, half * V_DIM

    def remote(src, dst, send, recv, sp=me, to=tp):
        return pltpu.make_async_remote_copy(
            src_ref=src, dst_ref=dst, send_sem=send, recv_sem=recv, device_id={"sp": sp, "tp": to}
        )

    def landed(ref, sem):
        pltpu.make_async_copy(ref, ref, sem).wait()

    own_kv = jnp.where(home, me, n)

    def slot_of(p):
        return jnp.where(home & (p == c), y, 2 + p)

    def load(k):
        if k < 2:
            return pltpu.make_async_copy(
                q_in_ref.at[:, pl.ds(k * pair_q, pair_q)], qb.at[slot_of(k)], load_sem.at[k]
            )
        src, dst = {
            2: (values_ref, kv.at[own_kv, 1]),
            3: (hidden_ref, hid_vm),
            4: (weight_ref, w_vm),
            5: (mo_in_ref, mo_vm),
            6: (og_in_ref, og_vm),
        }[k]
        return pltpu.make_async_copy(src, dst, load_sem.at[k])

    for k in (2, 0, 1, 3, 4, 5, 6):
        load(k).start()

    barrier = pltpu.get_barrier_semaphore()

    @pl.loop(1, n)
    def _(k):
        pl.semaphore_signal(barrier, inc=1, device_id={"sp": (me + k) % n})

    @pl.loop(1, tp_count)
    def _(k):
        pl.semaphore_signal(barrier, inc=1, device_id={"tp": (tp + k) % tp_count})

    pl.semaphore_signal(barrier, inc=1, device_id={"sp": mate, "tp": pair})
    pl.semaphore_wait(barrier, n + tp_count - 1)

    def spread(buf, p, send, recv):
        return remote(buf.at[2 + p], buf.at[y], send.at[p], recv.at[y], 2 * o + c, 2 * x + p)

    def not_self(p):
        return ~(home & (p == c))

    def arrive(buf, slot, recv):
        landed(buf.at[slot], recv.at[slot])

    def rows_arrive(slot):
        arrive(qb, slot, q_recv)
        arrive(db, slot, d_recv)
        arrive(mb, slot, m_recv)

    def own_copy(p):
        return remote(
            kv.at[own_kv, p], kv.at[me, p], kv_own.at[p], kv_recv.at[me, p],
            2 * o + c, 2 * x + jnp.where(home, 1 - c, p),
        )

    def up_copy(b):
        return remote(kv.at[b, c], kv.at[b, c], kv_up, kv_recv.at[b, c], me + 2)

    def pair_copy(b):
        return remote(kv.at[b, c], kv.at[b, c], kv_pair, kv_recv.at[b, c], me, pair)

    def kv_wait(b, p):
        landed(kv.at[b, p], kv_recv.at[b, p])

    def pass_up(b):
        @pl.when(has_up)
        def _():
            up_copy(b).start()

    def take(b):
        kv_wait(b, c)
        pass_up(b)
        pair_copy(b).start()

    part_rows = rows // tp_count
    wide = hid_vm.shape[1] // n
    own_rows = pl.ds(pl.multiple_of(tp * part_rows, part_rows), part_rows)

    def columns(dest):
        return pl.ds(pl.multiple_of(dest * wide, wide), wide)

    def hid_slice(dest):
        return remote(hid_vm.at[own_rows, columns(dest)], hid.at[tp, me], hid_send, hid_src.at[me], dest)

    def hid_down(first, last, side):
        @pl.loop(first, last)
        def _(l):
            hid_slice(2 * l + side).start()

    def hid_over(k, b):
        block = hid.at[tp, b]
        return remote(block, block, hid_pass.at[k], hid_recv.at[tp], me, (tp + 2 * k) % tp_count)

    def hid_cross(first, last, side):
        @pl.loop(first, last)
        def _(l):
            b = 2 * l + side

            @pl.when(b != me)
            def _():
                landed(hid.at[tp, b], hid_src.at[b])

            @pl.loop(1, tp_count // 2)
            def _(k):
                hid_over(k, b).start()

    def hid_to_pair(k):
        source = (tp + 2 * k) % tp_count
        return remote(hid.at[source], hid.at[source], hid_pair.at[k], hid_recv.at[source], me, pair)

    defer = ~home & ~has_up
    load(2).wait()

    @pl.when(~defer)
    def _():
        own_copy(1).start()

    @pl.when(home & (c == 1) & has_up)
    def _():
        up_copy(me).start()

    def send_q(p):
        load(p).wait()

        @pl.when(not_self(p))
        def _():
            spread(qb, p, q_send, q_recv).start()

    @pl.when(~has_up)
    def _():
        send_q(0)
        send_q(1)

    load(3).wait()
    load(4).wait()
    kv[own_kv, 0] = dot_nn(hid_vm[...], w_vm[...]).astype(jnp.bfloat16)

    @pl.when(~defer)
    def _():
        own_copy(0).start()

    @pl.when(home & (c == 0) & has_up)
    def _():
        up_copy(me).start()

    @pl.when(has_up)
    def _():
        send_q(0)
        send_q(1)

    load(5).wait()
    load(6).wait()

    @pl.loop(0, 2)
    def _(k):
        p = jnp.where(k == 0, 1 - c, c)
        head_terms(p, half, slot_of(p), og_vm, mo_vm, log_ref, mix_ref, gain_ref, db, mb)

        @pl.when(not_self(p))
        def _():
            spread(db, p, d_send, d_recv).start()
            spread(mb, p, m_send, m_recv).start()

    @pl.when(defer)
    def _():
        own_copy(1).start()
        own_copy(0).start()

    hid[tp, me] = hid_vm[own_rows, columns(me)]
    hid_down(0, o, y)

    @pl.when(~home)
    def _():
        hid_down(0, o + 1, 1 - y)

    gw_out[...] = jnp.zeros_like(gw_out)
    gq_t[...] = jnp.zeros_like(gq_t)

    def grads(b, slots, masked=False):
        grad_k, grad_v = block_grads(half, slots, kv.at[b, 0], kv.at[b, 1], qb, db, mb, gq_t, masked)
        return [(0, 0, grad_k[0]), (0, HEAD_DIM, grad_k[1]), (1, 0, grad_v)]

    def hold(at, pieces, add):
        for part, col, piece in pieces:
            cols = pl.ds(col, piece.shape[1])
            if add:
                acc[at, part, :, cols] += piece
            else:
                acc[at, part, :, cols] = piece

    def partial(b):
        return remote(p_out.at[b], p_in.at[b], p_send, p_recv.at[b], me, pair)

    def emit(b, pieces):
        for part, col, piece in pieces:
            cols = pl.ds(col, piece.shape[1])
            lo, hi = piece[:hrows], piece[hrows:]
            keep[b, part, :, cols] = jnp.where(c == 0, lo, hi)
            p_out[b, part, :, cols] = jnp.where(c == 0, hi, lo).astype(jnp.bfloat16)
        partial(b).start()

    def held(at):
        return [(part, 0, acc[at, part]) for part in range(2)]

    carried = jnp.where(home, c, 2)
    reach = 3

    def down(b, part):
        return remote(dn_out.at[b, part], up_in.at[b, part], dn_send, up_recv.at[b, part], me - 2)

    def gk_hop(b, sems, target):
        return remote(gkb.at[b, carried], gkb.at[b, carried], sems, gk_recv.at[b, 1], target)

    def gk_give(b, sems, target, to):
        return remote(gkb.at[b, carried], gkb.at[b, c], sems, gk_recv.at[b, 0], target, to)

    def gk_deliver(b, act):
        act(gk_give(b, gk_cross, mate, 2 * x + y))

        @pl.when(~home)
        def _():
            act(gk_give(b, gk_pair, me, pair))

    def gk_up_near(b):
        dist = (o - b // 2) % reach

        @pl.when(has_up & ((dist == 0) | ((dist == 1) & (o + 2 < outer))))
        def _():
            gk_hop(b, gk_up, me + 2).start()

    def gk_up_far(b):
        root = (o - b // 2) % reach == 0

        @pl.when(root & (o + 3 < outer))
        def _():
            gk_hop(b, gk_up, me + 6).start()

        @pl.when(root & (o + 3 == outer))
        def _():
            gk_hop(b, gk_up, me + 4).start()

    def gk_dn_hop(b, act):
        @pl.when(o > 0)
        def _():
            act(gk_hop(b, gk_dn, me - 2))

    def start(copy):
        copy.start()

    def gv_give(s):
        return remote(gv_fin.at[s], gv_in.at[c], gv_send.at[s], gv_recv.at[c], 2 * o + s, 2 * x + y)

    def each_of(level, act):
        @pl.loop(0, 2)
        def _(j):
            act(2 * level + jnp.where(j == 0, y, 1 - y))

    def reduce(b, part):
        if part == 0:
            landed(p_in.at[b], p_recv.at[b])

        @pl.when(has_up)
        def _():
            landed(up_in.at[b, part], up_recv.at[b, part])
            keep[b, part] += up_in[b, part].astype(jnp.float32)

        total = keep[b, part] + p_in[b, part].astype(jnp.float32)

        @pl.when(b // 2 < o)
        def _():
            dn_out[b, part] = total.astype(jnp.bfloat16)
            down(b, part).start()

        @pl.when(b // 2 == o)
        def _():
            if part == 0:
                gkb[b, carried] = (total * SCALE).astype(jnp.bfloat16)
                gk_up_near(b)

                @pl.when(b % 2 != y)
                def _():
                    each_of(o, gk_up_far)

                gk_dn_hop(b, start)
                gk_deliver(b, start)
            else:
                s = b % 2

                @pl.when(home & (s == y))
                def _():
                    gv_in[c] = total.astype(jnp.bfloat16)

                @pl.when(~(home & (s == y)))
                def _():
                    gv_fin[s] = total.astype(jnp.bfloat16)
                    gv_give(s).start()

    def sums(level, part):
        each_of(level, lambda b: reduce(b, part))

    @pl.when(~home)
    def _():
        kv_wait(me, c)
        pass_up(me)
        rows_arrive(y)
        kv_wait(me, 1 - c)

    hold(y, grads(me, [y], True), False)

    @pl.when(has_up)
    def _():
        take(mate)

    count = 2 * o

    def lower(i):
        return 2 * (o - 1 - i // 2) + jnp.where(i % 2 == 0, y, 1 - y)

    def take_lower(i):
        @pl.when(i < count)
        def _():
            take(lower(i))

    def top_reduce(i):
        @pl.when(~has_up)
        def _():
            reduce(lower(i), 0)

            @pl.when(i == 1)
            def _():
                reduce(lower(0), 1)
                reduce(lower(1), 1)

    ahead = jnp.minimum(count, jnp.where(has_up, 4, 2))

    @pl.loop(0, ahead)
    def _(i):
        b = lower(i)
        take(b)
        kv_wait(b, 1 - c)
        hold(2 + i, grads(b, [y]), False)

    @pl.when(~has_up)
    def _():
        take_lower(2)

    rows_arrive(1 - y)

    @pl.when(home)
    def _():
        hid_down(0, o + 1, 1 - y)

    def own_level():
        kv_wait(mate, 1 - c)
        hold(1 - y, grads(mate, [1 - y], True), False)
        top_reduce(count - 1)
        hold(0, grads(2 * o, [1]), True)
        emit(2 * o, held(0))
        emit(2 * o + 1, held(1))

    def hid_up():
        hid_down(o + 1, outer, y)
        hid_down(o + 1, outer, 1 - y)

    @pl.when(o == 0)
    def _():
        hid_up()

    @pl.when(has_up)
    def _():
        own_level()

    @pl.when(o > 0)
    def _():
        hid_up()

    below_top = has_up & near_top

    @pl.loop(0, ahead)
    def _(i):
        b = lower(i)
        hold(2 + i, grads(b, [1 - y]), True)
        emit(b, held(2 + i))

        @pl.when(i == 1)
        def _():
            top_reduce(0)

            @pl.when(below_top)
            def _():
                sums(o, 0)

    hid_cross(o, outer, y)

    @pl.when(has_up)
    def _():
        take_lower(4)
        take_lower(5)

    @pl.loop(ahead, count)
    def _(i):
        b = lower(i)
        kv_wait(b, 1 - c)
        emit(b, grads(b, [0, 1]))
        top_reduce(i - 1)

        @pl.when((i == 2) & ~has_up)
        def _():
            take_lower(3)

        take_lower(i + 2)

        @pl.when((i == count - 2) & ~has_up)
        def _():
            take(mate)

    @pl.when(~has_up)
    def _():
        @pl.when(count == 2)
        def _():
            take(mate)

        own_level()

        @pl.when(count > 2)
        def _():
            sums(0, 1)

    def gq_give(s):
        return remote(gq_fin.at[s], gq_in.at[c], gq_send.at[s], gq_recv.at[c], 2 * o + s, 2 * x + y)

    @pl.loop(0, 2)
    def _(k):
        s = jnp.where(k == 0, 1 - y, y)
        local = home & (s == y)
        for at in range(2 * half):
            cols = slice(at * HEAD_DIM, (at + 1) * HEAD_DIM)
            piece = (gq_t[s, cols, :] * SCALE).T.astype(jnp.bfloat16)

            @pl.when(local)
            def _():
                gq_in[c, :, cols] = piece

            @pl.when(~local)
            def _():
                gq_fin[s, :, cols] = piece

        @pl.when(~local)
        def _():
            gq_give(s).start()

    def hid_relay():
        hid_to_pair(0).start()

        @pl.loop(1, tp_count // 2)
        def _(k):
            source = (tp + 2 * k) % tp_count
            landed(hid.at[source], hid_recv.at[source])
            hid_to_pair(k).start()

    def hid_below(last):
        hid_cross(0, last, y)
        hid_cross(0, last, 1 - y)

    @pl.when(~near_top)
    def _():
        hid_cross(o, outer, 1 - y)
        hid_below(o)

    def gk_step(b):
        landed(gkb.at[b, carried], gk_recv.at[b, 1])

        @pl.when(b // 2 < o)
        def _():
            gk_up_near(b)
            gk_up_far(b)

        @pl.when(b // 2 > o)
        def _():
            gk_dn_hop(b, start)

        gk_deliver(b, start)

    def gk_ready(b):
        @pl.when(home)
        def _():
            landed(gkb.at[b, 0], gk_recv.at[b, 0])

        @pl.when(~home)
        def _():
            landed(gkb.at[b, pl.ds(0, 2)], gk_recv.at[b, 0])

    def add_weight(b):
        gk_ready(b)
        block = jnp.concatenate([hid[k, b] for k in range(tp_count)], axis=0)
        gw_out[...] += dot_tn(block, jnp.concatenate([gkb[b, 0], gkb[b, 1]], axis=0))

    def hid_finish():
        @pl.loop(0, tp_count // 2)
        def _(k):
            source = (pair + 2 * k) % tp_count
            landed(hid.at[source], hid_recv.at[source])

    def settle():
        for p in range(2):
            own_copy(p).wait_send()

            @pl.when(not_self(p))
            def _():
                spread(qb, p, q_send, q_recv).wait_send()
                spread(db, p, d_send, d_recv).wait_send()
                spread(mb, p, m_send, m_recv).wait_send()

            @pl.when(~(home & (y == p)))
            def _():
                gq_give(p).wait_send()

            @pl.when(~(home & (c == p)))
            def _():
                landed(gq_in.at[p], gq_recv.at[p])

            gq_out[:, p * pair_q : (p + 1) * pair_q] = gq_in[p]

        for l in range(outer):
            @pl.when(o == l)
            def _():
                if l < outer - 1:
                    landed(kv.at[pl.ds(0, 2 * l + 2), 0], kv_up)
                landed(kv.at[pl.ds(0, 2 * l + 1), 0], kv_pair)
                landed(p_out.at[pl.ds(0, 2 * l + 2)], p_send)

        landed(hid.at[tp, pl.ds(0, n - 1)], hid_send)

        @pl.loop(1, tp_count // 2)
        def _(k):
            landed(hid.at[tp], hid_pass.at[k])

    def finish():
        gk_out[:hrows] = gkb[me, 0]
        gk_out[hrows:] = gkb[me, 1]
        for h in range(2):
            @pl.when(~(home & (c == h)))
            def _():
                landed(gv_in.at[h], gv_recv.at[h])

            gv_out[h * hrows : (h + 1) * hrows] = gv_in[h]

            @pl.when(~(home & (y == h)))
            def _():
                gv_give(h).wait_send()

        for l in range(1, outer):
            @pl.when(o == l)
            def _():
                landed(dn_out.at[pl.ds(0, 2 * l)], dn_send)
                landed(gkb.at[pl.ds(0, n - 2 * l), 0], gk_dn)

        @pl.loop(0, tp_count // 2)
        def _(k):
            hid_to_pair(k).wait_send()

    first_up = jnp.where(near_top, o + 1, o + 2)

    @pl.when(o == 0)
    def _():
        hid_relay()

        @pl.loop(1, outer - 1)
        def _(l):
            each_of(l, gk_step)

        hid_finish()
        settle()

    @pl.when((o > 0) & ~near_top)
    def _():
        each_of(o + 1, gk_step)

    @pl.when(~below_top)
    def _():
        sums(o, 0)

    @pl.when(~has_up)
    def _():
        hid_cross(o, outer, 1 - y)
        hid_cross(o - 1, o, y)
        hid_cross(o - 1, o, 1 - y)

    @pl.when(o == 0)
    def _():
        @pl.loop(1, outer - 1)
        def _(l):
            each_of(l, add_weight)

    @pl.when((o == outer - 2) | (o == 0))
    def _():
        sums(o, 1)

    @pl.when(has_up & (o > 0))
    def _():
        @pl.loop(0, o)
        def _(k):
            sums(o - 1 - k, 0)

        @pl.when(near_top)
        def _():
            hid_cross(o, outer, 1 - y)
            hid_below(o)

        sums(0, 1)

    @pl.when(~has_up)
    def _():
        hid_below(o - 1)

    @pl.when((o == 1) & has_up)
    def _():
        hid_relay()

    @pl.loop(jnp.where(o == 0, outer - 1, first_up), outer)
    def _(l):
        each_of(l, gk_step)

    @pl.when((o == 1) & has_up)
    def _():
        each_of(0, gk_step)

    @pl.loop(1, jnp.where(has_up, o, o - 1))
    def _(l):
        sums(l, 1)

    @pl.when((o != outer - 2) & (o > 0))
    def _():
        sums(o, 1)

    @pl.loop(1, o)
    def _(k):
        each_of(o - k, gk_step)

    @pl.when((o > 1) | ~has_up)
    def _():
        hid_relay()

    @pl.when(o > 0)
    def _():
        hid_finish()
        settle()

        @pl.when((o > 1) | ~has_up)
        def _():
            each_of(0, gk_step)

        @pl.loop(1, outer)
        def _(k):
            each_of(jnp.where(k < outer - o + 1, o + k - 1, outer - k), add_weight)

    @pl.when(o == 0)
    def _():
        each_of(0, add_weight)

    finish()
    each_of(jnp.where(o == 0, outer - 1, 0), add_weight)

    for l in range(outer - 1):
        roots, nexts = l // reach + 1, (l - 1) // reach + 1
        hops = 2 * roots * min(2, outer - 1 - l) + 2 * nexts * (l + 2 < outer)

        @pl.when(o == l)
        def _():
            landed(gkb.at[pl.ds(0, hops), 0], gk_up)

    landed(gkb.at[pl.ds(0, n), 0], gk_cross)

    @pl.when(~home)
    def _():
        landed(gkb.at[pl.ds(0, n), 0], gk_pair)


def write_kernel(*refs):
    copies = [pltpu.make_async_copy(refs[k], refs[4 + k], refs[8].at[k]) for k in range(4)]
    for copy in copies:
        copy.start()
    for copy in copies:
        copy.wait()


def on_device(n, tp_count, hidden, key_weight, queries, values, map_out, log_sums, out_grad, mixing, out_gain):
    rows = queries.shape[0]
    heads = mixing.shape[0]
    width = values.shape[1]
    half = heads // 2
    hrows = rows // 2
    assert width == V_DIM and n % 2 == 0 and tp_count % 2 == 0 and n >= 4
    bf16, f32 = jnp.bfloat16, jnp.float32
    vm = pl.BlockSpec(memory_space=VMEM)
    hbm = pl.BlockSpec(memory_space=pl.ANY)
    buffers = [
        VMEM(hidden.shape, bf16),
        VMEM(key_weight.shape, bf16),
        VMEM(map_out.shape, bf16),
        VMEM(out_grad.shape, bf16),
        VMEM((4, rows, half * 2 * HEAD_DIM), bf16),
        VMEM((4, rows, half * V_DIM), bf16),
        VMEM((4, 4 * half, rows), f32),
        VMEM((n + 1, 2, rows, width), bf16),
        VMEM((6, 2, rows, width), f32),
        VMEM((n, 2, hrows, width), f32),
        VMEM((n, 2, hrows, width), bf16),
        VMEM((n, 2, hrows, width), bf16),
        VMEM((n, 2, hrows, width), bf16),
        VMEM((n, 2, hrows, width), bf16),
        VMEM((n, 3, hrows, width), bf16),
        VMEM((2, hrows, width), bf16),
        VMEM((2, hrows, width), bf16),
        VMEM((2, half * 2 * HEAD_DIM, rows), f32),
        VMEM((2, rows, half * 2 * HEAD_DIM), bf16),
        VMEM((2, rows, half * 2 * HEAD_DIM), bf16),
        VMEM((tp_count, n, rows // tp_count, hidden.shape[1] // n), bf16),
    ]
    sems = [
        DMA((7,)),
        *[DMA((2,))] * 6,
        DMA((n, 2)),
        DMA((2,)),
        *[DMA] * 3,
        DMA((n,)),
        DMA,
        DMA((n, 2)),
        DMA((n, 2)),
        *[DMA] * 4,
        *[DMA((2,))] * 4,
        DMA,
        DMA((n,)),
        DMA((tp_count,)),
        *[DMA((tp_count // 2,))] * 2,
    ]
    results = pl.pallas_call(
        functools.partial(attend_kernel, n, tp_count, heads),
        out_shape=(
            VMEM(queries.shape, bf16),
            VMEM((rows, width), bf16),
            VMEM((rows, width), bf16),
            VMEM((hidden.shape[1] // n, width), f32),
        ),
        in_specs=[hbm] * 6 + [vm] * 2 + [pl.BlockSpec(memory_space=pltpu.SMEM)],
        out_specs=(vm, vm, vm, vm),
        scratch_shapes=buffers + sems,
        compiler_params=pltpu.CompilerParams(
            vmem_limit_bytes=60 * 2**20, collective_id=0, has_side_effects=True
        ),
        cost_estimate=pl.CostEstimate(flops=5 * 10**9, bytes_accessed=10**7, transcendentals=0),
    )(hidden, key_weight, values, queries, map_out, out_grad, log_sums, out_gain.reshape(1, V_DIM), mixing)
    return pl.pallas_call(
        write_kernel,
        out_shape=tuple(jax.ShapeDtypeStruct(r.shape, r.dtype) for r in results),
        in_specs=[vm] * 4,
        out_specs=(hbm,) * 4,
        scratch_shapes=[DMA((4,))],
        cost_estimate=pl.CostEstimate(flops=10**6, bytes_accessed=4 * 10**6, transcendentals=0),
    )(*[pltpu.with_memory_space_constraint(r, VMEM) for r in results])


def solution(mesh):
    placed = (
        P("sp", None),
        P(None, "tp"),
        P("sp", "tp"),
        P("sp", "tp"),
        P("sp", "tp"),
        P("tp", "sp"),
        P("sp", "tp"),
        P("tp"),
        P(),
    )
    return jax.shard_map(
        functools.partial(on_device, mesh.shape["sp"], mesh.shape["tp"]),
        mesh=mesh,
        in_specs=placed,
        out_specs=(P("sp", "tp"), P("sp", "tp"), P("sp", "tp"), P("sp", "tp")),
        check_vma=False,
    )
```

```python
import functools
import math

import jax
import jax.numpy as jnp
from jax import lax
from jax.experimental import pallas as pl
from jax.experimental.pallas import tpu as pltpu
from jax.sharding import PartitionSpec as P

HEAD_DIM = 128
V_DIM = 256
OUT_SCALE = 0.8
NORM_EPS = 1e-06
LOG2E = math.log2(math.e)
SCALE = HEAD_DIM ** (-0.5)
VMEM = pltpu.VMEM
DMA = pltpu.SemaphoreType.DMA


def dot_nn(a, b):
    return lax.dot_general(a, b, (((1,), (0,)), ((), ())), preferred_element_type=jnp.float32)


def dot_nt(a, b):
    return lax.dot_general(a, b, (((1,), (1,)), ((), ())), preferred_element_type=jnp.float32)


def dot_tn(a, b):
    return lax.dot_general(a, b, (((0,), (0,)), ((), ())), preferred_element_type=jnp.float32)


def head_terms(pair, half, slot, og_ref, mo_ref, log_ref, mix_ref, gain_ref, d_ref, m_ref):
    gain = gain_ref[...] * OUT_SCALE
    rows = og_ref.shape[0]
    cols, lifts = [], []
    for i in range(half):
        h = pair * half + i
        at = pl.multiple_of(2 * h * V_DIM, V_DIM)
        map_a = mo_ref[:, pl.ds(at, V_DIM)].astype(jnp.float32)
        map_b = mo_ref[:, pl.ds(at + V_DIM, V_DIM)].astype(jnp.float32)
        pre = map_a - mix_ref[h] * map_b
        inv = lax.rsqrt(jnp.mean(pre * pre, axis=-1, keepdims=True) + NORM_EPS)
        up = og_ref[:, pl.ds(pl.multiple_of(h * V_DIM, V_DIM), V_DIM)].astype(jnp.float32) * gain
        d_out = inv * (up - pre * (inv * inv * jnp.mean(up * pre, axis=-1, keepdims=True)))
        d_ref[slot, :, i * V_DIM : (i + 1) * V_DIM] = d_out.astype(jnp.bfloat16)
        cols.append(jnp.sum(d_out * map_a, axis=-1, keepdims=True))
        cols.append(jnp.sum(d_out * map_b, axis=-1, keepdims=True))
        lifts.append(jnp.zeros((1, rows), jnp.float32))
        lifts.append(jnp.log(jnp.full((1, rows), mix_ref[h], jnp.float32)))
    lane = lax.broadcasted_iota(jnp.int32, (rows, 128), 1)
    packed = jnp.zeros((rows, 128), jnp.float32)
    for at, col in enumerate(cols):
        packed = jnp.where(lane == at, col, packed)
    logs = log_ref[...]
    logs = jnp.where(pair == 0, logs[: 2 * half], logs[2 * half :])
    m_ref[slot, : 2 * half] = (logs - jnp.concatenate(lifts, axis=0)) * LOG2E
    m_ref[slot, 2 * half :] = packed.T[: 2 * half]


def block_grads(half, slots, k_ref, v_ref, q_ref, d_ref, m_ref, gq_ref, masked):
    keys = [k_ref[:, m * HEAD_DIM : (m + 1) * HEAD_DIM] for m in range(2)]
    keys_t = [k.T for k in keys]
    vals = v_ref[...]
    grad_k = [None, None]
    grad_v = None
    for slot in slots:
        for i in range(half):
            d_h = d_ref[slot, :, i * V_DIM : (i + 1) * V_DIM]
            d_attn = dot_nt(vals, d_h)
            qs, probs, terms = [], [], []
            for m in range(2):
                at = 2 * i + m
                q = q_ref[slot, :, at * HEAD_DIM : (at + 1) * HEAD_DIM]
                p = jnp.exp2(dot_nt(keys[m], q) * (SCALE * LOG2E) - m_ref[slot, at : at + 1, :])
                if masked:
                    k_at = lax.broadcasted_iota(jnp.int32, p.shape, 0)
                    q_at = lax.broadcasted_iota(jnp.int32, p.shape, 1)
                    p = jnp.where(k_at <= q_at, p, 0.0)
                qs.append(q)
                probs.append(p)
                terms.append(m_ref[slot, 2 * half + at : 2 * half + at + 1, :])
            w = (probs[0] - probs[1]).astype(jnp.bfloat16)
            ds = [
                (probs[0] * (d_attn - terms[0])).astype(jnp.bfloat16),
                (probs[1] * (terms[1] - d_attn)).astype(jnp.bfloat16),
            ]
            for m in range(2):
                at = 2 * i + m
                gq_ref[slot, at * HEAD_DIM : (at + 1) * HEAD_DIM, :] += dot_nn(keys_t[m], ds[m])
                gk = dot_nn(ds[m], qs[m])
                grad_k[m] = gk if grad_k[m] is None else grad_k[m] + gk
            gv = dot_nn(w, d_h)
            grad_v = gv if grad_v is None else grad_v + gv
    return grad_k, grad_v


def attend_kernel(
    n, tp_count, heads,
    hidden_ref, weight_ref, values_ref, q_in_ref, mo_in_ref, og_in_ref, log_ref, gain_ref, mix_ref,
    gq_out, gk_out, gv_out, gw_out,
    hid_vm, w_vm, mo_vm, og_vm, qb, db, mb, kv, acc, keep, p_out, p_in, up_in, dn_out,
    gkb, gv_fin, gv_in, gq_t, gq_fin, gq_in, hid,
    load_sem, q_send, q_recv, d_send, d_recv, m_send, m_recv,
    kv_recv, kv_own, kv_up, kv_pair, p_send, p_recv, dn_send, up_recv,
    gk_recv, gk_up, gk_dn, gk_pair, gk_cross, gv_send, gv_recv, gq_send, gq_recv,
    hid_send, hid_src, hid_recv, hid_pass, hid_pair,
):
    me = lax.axis_index("sp")
    tp = lax.axis_index("tp")
    outer = n // 2
    half = heads // 2
    o, y = me // 2, me % 2
    x, c = tp // 2, tp % 2
    mate, pair = me + 1 - 2 * y, tp + 1 - 2 * c
    has_up = o < outer - 1
    near_top = o >= outer - 2
    home = y == c
    rows = og_in_ref.shape[0]
    hrows = rows // 2
    pair_q, pair_v = half * 2 * HEAD_DIM, half * V_DIM

    def remote(src, dst, send, recv, sp=me, to=tp):
        return pltpu.make_async_remote_copy(
            src_ref=src, dst_ref=dst, send_sem=send, recv_sem=recv, device_id={"sp": sp, "tp": to}
        )

    def landed(ref, sem):
        pltpu.make_async_copy(ref, ref, sem).wait()

    own_kv = jnp.where(home, me, n)

    def slot_of(p):
        return jnp.where(home & (p == c), y, 2 + p)

    def load(k):
        if k < 2:
            return pltpu.make_async_copy(
                q_in_ref.at[:, pl.ds(k * pair_q, pair_q)], qb.at[slot_of(k)], load_sem.at[k]
            )
        src, dst = {
            2: (values_ref, kv.at[own_kv, 1]),
            3: (hidden_ref, hid_vm),
            4: (weight_ref, w_vm),
            5: (mo_in_ref, mo_vm),
            6: (og_in_ref, og_vm),
        }[k]
        return pltpu.make_async_copy(src, dst, load_sem.at[k])

    for k in (2, 0, 1, 3, 4, 5, 6):
        load(k).start()

    barrier = pltpu.get_barrier_semaphore()

    @pl.loop(1, n)
    def _(k):
        pl.semaphore_signal(barrier, inc=1, device_id={"sp": (me + k) % n})

    @pl.loop(1, tp_count)
    def _(k):
        pl.semaphore_signal(barrier, inc=1, device_id={"tp": (tp + k) % tp_count})

    pl.semaphore_signal(barrier, inc=1, device_id={"sp": mate, "tp": pair})
    pl.semaphore_wait(barrier, n + tp_count - 1)

    def spread(buf, p, send, recv):
        return remote(buf.at[2 + p], buf.at[y], send.at[p], recv.at[y], 2 * o + c, 2 * x + p)

    def not_self(p):
        return ~(home & (p == c))

    def arrive(buf, slot, recv):
        landed(buf.at[slot], recv.at[slot])

    def rows_arrive(slot):
        arrive(qb, slot, q_recv)
        arrive(db, slot, d_recv)
        arrive(mb, slot, m_recv)

    def own_copy(p):
        return remote(
            kv.at[own_kv, p], kv.at[me, p], kv_own.at[p], kv_recv.at[me, p],
            2 * o + c, 2 * x + jnp.where(home, 1 - c, p),
        )

    def up_copy(b):
        return remote(kv.at[b, c], kv.at[b, c], kv_up, kv_recv.at[b, c], me + 2)

    def pair_copy(b):
        return remote(kv.at[b, c], kv.at[b, c], kv_pair, kv_recv.at[b, c], me, pair)

    def kv_wait(b, p):
        landed(kv.at[b, p], kv_recv.at[b, p])

    def pass_up(b):
        @pl.when(has_up)
        def _():
            up_copy(b).start()

    def take(b):
        kv_wait(b, c)
        pass_up(b)
        pair_copy(b).start()

    part_rows = rows // tp_count
    wide = hid_vm.shape[1] // n
    own_rows = pl.ds(pl.multiple_of(tp * part_rows, part_rows), part_rows)

    def columns(dest):
        return pl.ds(pl.multiple_of(dest * wide, wide), wide)

    def hid_slice(dest):
        return remote(hid_vm.at[own_rows, columns(dest)], hid.at[tp, me], hid_send, hid_src.at[me], dest)

    def hid_down(first, last, side):
        @pl.loop(first, last)
        def _(l):
            hid_slice(2 * l + side).start()

    def hid_over(k, b):
        block = hid.at[tp, b]
        return remote(block, block, hid_pass.at[k], hid_recv.at[tp], me, (tp + 2 * k) % tp_count)

    def hid_cross(first, last, side):
        @pl.loop(first, last)
        def _(l):
            b = 2 * l + side

            @pl.when(b != me)
            def _():
                landed(hid.at[tp, b], hid_src.at[b])

            @pl.loop(1, tp_count // 2)
            def _(k):
                hid_over(k, b).start()

    def hid_to_pair(k):
        source = (tp + 2 * k) % tp_count
        return remote(hid.at[source], hid.at[source], hid_pair.at[k], hid_recv.at[source], me, pair)

    defer = ~home & ~has_up
    load(2).wait()

    @pl.when(~defer)
    def _():
        own_copy(1).start()

    @pl.when(home & (c == 1) & has_up)
    def _():
        up_copy(me).start()

    def send_q(p):
        load(p).wait()

        @pl.when(not_self(p))
        def _():
            spread(qb, p, q_send, q_recv).start()

    @pl.when(~has_up)
    def _():
        send_q(0)
        send_q(1)

    load(3).wait()
    load(4).wait()
    kv[own_kv, 0] = dot_nn(hid_vm[...], w_vm[...]).astype(jnp.bfloat16)

    @pl.when(~defer)
    def _():
        own_copy(0).start()

    @pl.when(home & (c == 0) & has_up)
    def _():
        up_copy(me).start()

    @pl.when(has_up)
    def _():
        send_q(0)
        send_q(1)

    load(5).wait()
    load(6).wait()

    @pl.loop(0, 2)
    def _(k):
        p = jnp.where(k == 0, 1 - c, c)
        head_terms(p, half, slot_of(p), og_vm, mo_vm, log_ref, mix_ref, gain_ref, db, mb)

        @pl.when(not_self(p))
        def _():
            spread(db, p, d_send, d_recv).start()
            spread(mb, p, m_send, m_recv).start()

    @pl.when(defer)
    def _():
        own_copy(1).start()
        own_copy(0).start()

    hid[tp, me] = hid_vm[own_rows, columns(me)]
    hid_down(0, o, y)

    @pl.when(~home)
    def _():
        hid_down(0, o + 1, 1 - y)

    gw_out[...] = jnp.zeros_like(gw_out)
    gq_t[...] = jnp.zeros_like(gq_t)

    def grads(b, slots, masked=False):
        grad_k, grad_v = block_grads(half, slots, kv.at[b, 0], kv.at[b, 1], qb, db, mb, gq_t, masked)
        return [(0, 0, grad_k[0]), (0, HEAD_DIM, grad_k[1]), (1, 0, grad_v)]

    def hold(at, pieces, add):
        for part, col, piece in pieces:
            cols = pl.ds(col, piece.shape[1])
            if add:
                acc[at, part, :, cols] += piece
            else:
                acc[at, part, :, cols] = piece

    def partial(b):
        return remote(p_out.at[b], p_in.at[b], p_send, p_recv.at[b], me, pair)

    def emit(b, pieces):
        for part, col, piece in pieces:
            cols = pl.ds(col, piece.shape[1])
            lo, hi = piece[:hrows], piece[hrows:]
            keep[b, part, :, cols] = jnp.where(c == 0, lo, hi)
            p_out[b, part, :, cols] = jnp.where(c == 0, hi, lo).astype(jnp.bfloat16)
        partial(b).start()

    def held(at):
        return [(part, 0, acc[at, part]) for part in range(2)]

    carried = jnp.where(home, c, 2)
    reach = 3

    def sub_rows(sub):
        return pl.ds(sub * (hrows // 2), hrows // 2)

    def down(b, part, sub):
        rows_at = sub_rows(sub) if part == 0 else pl.ds(0, hrows)
        at = sub if part == 0 else 2
        return remote(
            dn_out.at[b, part, rows_at], up_in.at[b, part, rows_at], dn_send, up_recv.at[b, at], me - 2
        )

    def gk_hop(b, sub, sems, target):
        piece = gkb.at[b, carried, sub_rows(sub)]
        return remote(piece, piece, sems, gk_recv.at[b, 1 + sub], target)

    def gk_give(b, sub, sems, target, to):
        return remote(
            gkb.at[b, carried, sub_rows(sub)], gkb.at[b, c, sub_rows(sub)], sems, gk_recv.at[b, 0], target, to
        )

    def gk_deliver(b, sub):
        gk_give(b, sub, gk_cross, mate, 2 * x + y).start()

        @pl.when(~home)
        def _():
            gk_give(b, sub, gk_pair, me, pair).start()

    def gk_up_near(b, sub):
        dist = (o - b // 2) % reach

        @pl.when(has_up & ((dist == 0) | ((dist == 1) & (o + 2 < outer))))
        def _():
            gk_hop(b, sub, gk_up, me + 2).start()

    def gk_up_far(b):
        root = (o - b // 2) % reach == 0

        for sub in range(2):
            @pl.when(root & (o + 3 < outer))
            def _():
                gk_hop(b, sub, gk_up, me + 6).start()

            @pl.when(root & (o + 3 == outer))
            def _():
                gk_hop(b, sub, gk_up, me + 4).start()

    def gk_dn_hop(b, sub):
        @pl.when(o > 0)
        def _():
            gk_hop(b, sub, gk_dn, me - 2).start()

    def gv_give(s):
        return remote(gv_fin.at[s], gv_in.at[c], gv_send.at[s], gv_recv.at[c], 2 * o + s, 2 * x + y)

    def each_of(level, act):
        @pl.loop(0, 2)
        def _(j):
            act(2 * level + jnp.where(j == 0, y, 1 - y))

    def reduce(b, part):
        if part == 0:
            landed(p_in.at[b], p_recv.at[b])

        for sub in range(2 if part == 0 else 1):
            rows_at = sub_rows(sub) if part == 0 else pl.ds(0, hrows)

            @pl.when(has_up)
            def _():
                landed(up_in.at[b, part, rows_at], up_recv.at[b, sub if part == 0 else 2])
                keep[b, part, rows_at] += up_in[b, part, rows_at].astype(jnp.float32)

            total = keep[b, part, rows_at] + p_in[b, part, rows_at].astype(jnp.float32)

            @pl.when(b // 2 < o)
            def _():
                dn_out[b, part, rows_at] = total.astype(jnp.bfloat16)
                down(b, part, sub).start()

            @pl.when(b // 2 == o)
            def _():
                if part == 0:
                    gkb[b, carried, rows_at] = (total * SCALE).astype(jnp.bfloat16)
                    gk_up_near(b, sub)

                    if sub == 1:
                        @pl.when(b % 2 != y)
                        def _():
                            each_of(o, gk_up_far)

                    gk_dn_hop(b, sub)
                    gk_deliver(b, sub)
                else:
                    s = b % 2

                    @pl.when(home & (s == y))
                    def _():
                        gv_in[c] = total.astype(jnp.bfloat16)

                    @pl.when(~(home & (s == y)))
                    def _():
                        gv_fin[s] = total.astype(jnp.bfloat16)
                        gv_give(s).start()

    def sums(level, part):
        each_of(level, lambda b: reduce(b, part))

    @pl.when(~home)
    def _():
        kv_wait(me, c)
        pass_up(me)
        rows_arrive(y)
        kv_wait(me, 1 - c)

    hold(y, grads(me, [y], True), False)

    @pl.when(has_up)
    def _():
        take(mate)

    count = 2 * o

    def lower(i):
        return 2 * (o - 1 - i // 2) + jnp.where(i % 2 == 0, y, 1 - y)

    def take_lower(i):
        @pl.when(i < count)
        def _():
            take(lower(i))

    def top_reduce(i):
        @pl.when(~has_up)
        def _():
            reduce(lower(i), 0)

            @pl.when(i == 1)
            def _():
                reduce(lower(0), 1)
                reduce(lower(1), 1)

    ahead = jnp.minimum(count, jnp.where(has_up, 4, 2))

    @pl.loop(0, ahead)
    def _(i):
        b = lower(i)
        take(b)
        kv_wait(b, 1 - c)
        hold(2 + i, grads(b, [y]), False)

    @pl.when(~has_up)
    def _():
        take_lower(2)

    rows_arrive(1 - y)

    @pl.when(home)
    def _():
        hid_down(0, o + 1, 1 - y)

    def gq_give(s):
        return remote(gq_fin.at[s], gq_in.at[c], gq_send.at[s], gq_recv.at[c], 2 * o + s, 2 * x + y)

    def gq_part(k):
        s = jnp.where(k == 0, 1 - y, y)
        local = home & (s == y)
        for at in range(2 * half):
            cols = slice(at * HEAD_DIM, (at + 1) * HEAD_DIM)
            piece = (gq_t[s, cols, :] * SCALE).T.astype(jnp.bfloat16)

            @pl.when(local)
            def _():
                gq_in[c, :, cols] = piece

            @pl.when(~local)
            def _():
                gq_fin[s, :, cols] = piece

        @pl.when(~local)
        def _():
            gq_give(s).start()

    def own_level():
        kv_wait(mate, 1 - c)
        hold(1 - y, grads(mate, [1 - y], True), False)
        top_reduce(count - 1)
        hold(0, grads(2 * o, [1]), True)

        @pl.when(~has_up)
        def _():
            gq_part(0)

        emit(2 * o, held(0))
        emit(2 * o + 1, held(1))

    def hid_up():
        hid_down(o + 1, outer, y)
        hid_down(o + 1, outer, 1 - y)

    @pl.when(o == 0)
    def _():
        hid_up()

    @pl.when(has_up)
    def _():
        own_level()

    @pl.when(o > 0)
    def _():
        hid_up()

    below_top = has_up & near_top

    @pl.loop(0, ahead)
    def _(i):
        b = lower(i)
        hold(2 + i, grads(b, [1 - y]), True)
        emit(b, held(2 + i))

        @pl.when(i == 1)
        def _():
            top_reduce(0)

            @pl.when(below_top)
            def _():
                sums(o, 0)

    hid_cross(o, outer, y)

    @pl.when(has_up)
    def _():
        take_lower(4)
        take_lower(5)

    @pl.loop(ahead, count)
    def _(i):
        b = lower(i)
        kv_wait(b, 1 - c)
        emit(b, grads(b, [0, 1]))
        top_reduce(i - 1)

        @pl.when((i == 2) & ~has_up)
        def _():
            take_lower(3)

        take_lower(i + 2)

        @pl.when((i == count - 2) & ~has_up)
        def _():
            take(mate)

    @pl.when(~has_up)
    def _():
        @pl.when(count == 2)
        def _():
            take(mate)

        own_level()

        @pl.when(count > 2)
        def _():
            sums(0, 1)

    @pl.loop(jnp.where(has_up, 0, 1), 2)
    def _(k):
        gq_part(k)

    def hid_relay():
        hid_to_pair(0).start()

        @pl.loop(1, tp_count // 2)
        def _(k):
            source = (tp + 2 * k) % tp_count
            landed(hid.at[source], hid_recv.at[source])
            hid_to_pair(k).start()

    def hid_below(last):
        hid_cross(0, last, y)
        hid_cross(0, last, 1 - y)

    @pl.when(~near_top)
    def _():
        hid_cross(o, outer, 1 - y)
        hid_below(o)

    def gk_step(b):
        for sub in range(2):
            landed(gkb.at[b, carried, sub_rows(sub)], gk_recv.at[b, 1 + sub])

            @pl.when(b // 2 < o)
            def _():
                gk_up_near(b, sub)

            @pl.when(b // 2 > o)
            def _():
                gk_dn_hop(b, sub)

            gk_deliver(b, sub)

        @pl.when(b // 2 < o)
        def _():
            gk_up_far(b)

    def gk_ready(b):
        @pl.when(home)
        def _():
            landed(gkb.at[b, 0], gk_recv.at[b, 0])

        @pl.when(~home)
        def _():
            landed(gkb.at[b, pl.ds(0, 2)], gk_recv.at[b, 0])

    def add_weight(b):
        gk_ready(b)
        block = jnp.concatenate([hid[k, b] for k in range(tp_count)], axis=0)
        gw_out[...] += dot_tn(block, jnp.concatenate([gkb[b, 0], gkb[b, 1]], axis=0))

    def hid_finish():
        @pl.loop(0, tp_count // 2)
        def _(k):
            source = (pair + 2 * k) % tp_count
            landed(hid.at[source], hid_recv.at[source])

    def settle():
        for p in range(2):
            own_copy(p).wait_send()

            @pl.when(not_self(p))
            def _():
                spread(qb, p, q_send, q_recv).wait_send()
                spread(db, p, d_send, d_recv).wait_send()
                spread(mb, p, m_send, m_recv).wait_send()

            @pl.when(~(home & (y == p)))
            def _():
                gq_give(p).wait_send()

            @pl.when(~(home & (c == p)))
            def _():
                landed(gq_in.at[p], gq_recv.at[p])

            gq_out[:, p * pair_q : (p + 1) * pair_q] = gq_in[p]

        for l in range(outer):
            @pl.when(o == l)
            def _():
                if l < outer - 1:
                    landed(kv.at[pl.ds(0, 2 * l + 2), 0], kv_up)
                landed(kv.at[pl.ds(0, 2 * l + 1), 0], kv_pair)
                landed(p_out.at[pl.ds(0, 2 * l + 2)], p_send)

        landed(hid.at[tp, pl.ds(0, n - 1)], hid_send)

        @pl.loop(1, tp_count // 2)
        def _(k):
            landed(hid.at[tp], hid_pass.at[k])

    def finish():
        gk_out[:hrows] = gkb[me, 0]
        gk_out[hrows:] = gkb[me, 1]
        for h in range(2):
            @pl.when(~(home & (c == h)))
            def _():
                landed(gv_in.at[h], gv_recv.at[h])

            gv_out[h * hrows : (h + 1) * hrows] = gv_in[h]

            @pl.when(~(home & (y == h)))
            def _():
                gv_give(h).wait_send()

        for l in range(1, outer):
            @pl.when(o == l)
            def _():
                landed(dn_out.at[pl.ds(0, 2 * l)], dn_send)
                landed(gkb.at[pl.ds(0, n - 2 * l), 0], gk_dn)

        @pl.loop(0, tp_count // 2)
        def _(k):
            hid_to_pair(k).wait_send()

    first_up = jnp.where(near_top, o + 1, o + 2)

    @pl.when(o == 0)
    def _():
        hid_relay()

        @pl.loop(1, outer - 1)
        def _(l):
            each_of(l, gk_step)

        hid_finish()
        settle()

    @pl.when((o > 0) & ~near_top)
    def _():
        each_of(o + 1, gk_step)

    @pl.when(~below_top)
    def _():
        sums(o, 0)

    @pl.when(~has_up)
    def _():
        hid_cross(o, outer, 1 - y)
        hid_cross(o - 1, o, y)
        hid_cross(o - 1, o, 1 - y)

    @pl.when(o == 0)
    def _():
        @pl.loop(1, outer - 1)
        def _(l):
            each_of(l, add_weight)

    @pl.when((o == outer - 2) | (o == 0))
    def _():
        sums(o, 1)

    @pl.when(has_up & (o > 0))
    def _():
        @pl.loop(0, o)
        def _(k):
            sums(o - 1 - k, 0)

        @pl.when(near_top)
        def _():
            hid_cross(o, outer, 1 - y)
            hid_below(o)

        sums(0, 1)

    @pl.when(~has_up)
    def _():
        hid_below(o - 1)

    @pl.when((o == 1) & has_up)
    def _():
        hid_relay()

    @pl.loop(jnp.where(o == 0, outer - 1, first_up), outer)
    def _(l):
        each_of(l, gk_step)

    @pl.when((o == 1) & has_up)
    def _():
        each_of(0, gk_step)

    @pl.loop(1, jnp.where(has_up, o, o - 1))
    def _(l):
        sums(l, 1)

    @pl.when((o != outer - 2) & (o > 0))
    def _():
        sums(o, 1)

    @pl.loop(1, o)
    def _(k):
        each_of(o - k, gk_step)

    @pl.when((o > 1) | ~has_up)
    def _():
        hid_relay()

    @pl.when(o > 0)
    def _():
        hid_finish()
        settle()

        @pl.when((o > 1) | ~has_up)
        def _():
            each_of(0, gk_step)

        @pl.loop(1, outer)
        def _(k):
            each_of(jnp.where(k < outer - o + 1, o + k - 1, outer - k), add_weight)

    @pl.when(o == 0)
    def _():
        each_of(0, add_weight)

    finish()
    each_of(jnp.where(o == 0, outer - 1, 0), add_weight)

    for l in range(outer - 1):
        roots, nexts = l // reach + 1, (l - 1) // reach + 1
        hops = 2 * roots * min(2, outer - 1 - l) + 2 * nexts * (l + 2 < outer)

        @pl.when(o == l)
        def _():
            landed(gkb.at[pl.ds(0, hops), 0], gk_up)

    landed(gkb.at[pl.ds(0, n), 0], gk_cross)

    @pl.when(~home)
    def _():
        landed(gkb.at[pl.ds(0, n), 0], gk_pair)


def write_kernel(*refs):
    copies = [pltpu.make_async_copy(refs[k], refs[4 + k], refs[8].at[k]) for k in range(4)]
    for copy in copies:
        copy.start()
    for copy in copies:
        copy.wait()


def on_device(n, tp_count, hidden, key_weight, queries, values, map_out, log_sums, out_grad, mixing, out_gain):
    rows = queries.shape[0]
    heads = mixing.shape[0]
    width = values.shape[1]
    half = heads // 2
    hrows = rows // 2
    assert width == V_DIM and n % 2 == 0 and tp_count % 2 == 0 and n >= 4
    bf16, f32 = jnp.bfloat16, jnp.float32
    vm = pl.BlockSpec(memory_space=VMEM)
    hbm = pl.BlockSpec(memory_space=pl.ANY)
    buffers = [
        VMEM(hidden.shape, bf16),
        VMEM(key_weight.shape, bf16),
        VMEM(map_out.shape, bf16),
        VMEM(out_grad.shape, bf16),
        VMEM((4, rows, half * 2 * HEAD_DIM), bf16),
        VMEM((4, rows, half * V_DIM), bf16),
        VMEM((4, 4 * half, rows), f32),
        VMEM((n + 1, 2, rows, width), bf16),
        VMEM((6, 2, rows, width), f32),
        VMEM((n, 2, hrows, width), f32),
        VMEM((n, 2, hrows, width), bf16),
        VMEM((n, 2, hrows, width), bf16),
        VMEM((n, 2, hrows, width), bf16),
        VMEM((n, 2, hrows, width), bf16),
        VMEM((n, 3, hrows, width), bf16),
        VMEM((2, hrows, width), bf16),
        VMEM((2, hrows, width), bf16),
        VMEM((2, half * 2 * HEAD_DIM, rows), f32),
        VMEM((2, rows, half * 2 * HEAD_DIM), bf16),
        VMEM((2, rows, half * 2 * HEAD_DIM), bf16),
        VMEM((tp_count, n, rows // tp_count, hidden.shape[1] // n), bf16),
    ]
    sems = [
        DMA((7,)),
        *[DMA((2,))] * 6,
        DMA((n, 2)),
        DMA((2,)),
        *[DMA] * 3,
        DMA((n,)),
        DMA,
        DMA((n, 3)),
        DMA((n, 3)),
        *[DMA] * 4,
        *[DMA((2,))] * 4,
        DMA,
        DMA((n,)),
        DMA((tp_count,)),
        *[DMA((tp_count // 2,))] * 2,
    ]
    results = pl.pallas_call(
        functools.partial(attend_kernel, n, tp_count, heads),
        out_shape=(
            VMEM(queries.shape, bf16),
            VMEM((rows, width), bf16),
            VMEM((rows, width), bf16),
            VMEM((hidden.shape[1] // n, width), f32),
        ),
        in_specs=[hbm] * 6 + [vm] * 2 + [pl.BlockSpec(memory_space=pltpu.SMEM)],
        out_specs=(vm, vm, vm, vm),
        scratch_shapes=buffers + sems,
        compiler_params=pltpu.CompilerParams(
            vmem_limit_bytes=60 * 2**20, collective_id=0, has_side_effects=True
        ),
        cost_estimate=pl.CostEstimate(flops=5 * 10**9, bytes_accessed=10**7, transcendentals=0),
    )(hidden, key_weight, values, queries, map_out, out_grad, log_sums, out_gain.reshape(1, V_DIM), mixing)
    return pl.pallas_call(
        write_kernel,
        out_shape=tuple(jax.ShapeDtypeStruct(r.shape, r.dtype) for r in results),
        in_specs=[vm] * 4,
        out_specs=(hbm,) * 4,
        scratch_shapes=[DMA((4,))],
        cost_estimate=pl.CostEstimate(flops=10**6, bytes_accessed=4 * 10**6, transcendentals=0),
    )(*[pltpu.with_memory_space_constraint(r, VMEM) for r in results])


def solution(mesh):
    placed = (
        P("sp", None),
        P(None, "tp"),
        P("sp", "tp"),
        P("sp", "tp"),
        P("sp", "tp"),
        P("tp", "sp"),
        P("sp", "tp"),
        P("tp"),
        P(),
    )
    return jax.shard_map(
        functools.partial(on_device, mesh.shape["sp"], mesh.shape["tp"]),
        mesh=mesh,
        in_specs=placed,
        out_specs=(P("sp", "tp"), P("sp", "tp"), P("sp", "tp"), P("sp", "tp")),
        check_vma=False,
    )
```
